256 devices in a mesh: grp: 2 (over y), ep: 64 (over z, x), tp: 2 (over core).
Axes of the slice: x: 4, y: 2, z: 16, core: 2. Of those that a mesh axis runs over, the one named last changes fastest.
The devices are a block of a 4x16x16 slice.
Arguments:
- hidden: bfloat16 [1024, 2048], P(('grp', 'ep'), 'tp'), parts along dimension 0, may hold values from -6 to 6
- head_input_projected: bfloat16 [1024, 2048], P(('grp', 'ep'), 'tp'), parts along dimension 0, may hold values from -6 to 6
- output_gate_projected: bfloat16 [1024, 2048], P(('grp', 'ep'), 'tp'), parts along dimension 0, may hold values from -6 to 6
- input_map_projected: bfloat16 [1024, 256], P(('grp', 'ep'), 'tp'), parts along dimension 0, may hold values from -0.59765625 to 0.59765625
- output_map_projected: bfloat16 [1024, 256], P(('grp', 'ep'), 'tp'), parts along dimension 0, may hold values from -6 to 6
- raw_step_size: bfloat16 [1024, 32], P(('grp', 'ep'), 'tp'), parts along dimension 0, may hold values from -5 to 5
- convolution_history: bfloat16 [1024, 3, 2048], P(('grp', 'ep'), None, 'tp'), parts along dimension 0, may hold values from -6 to 6
- convolution_kernel: bfloat16 [4, 2048], P(None, 'tp'), may hold values from -3 to 3
- recurrent_state_matrix: float32 [1024, 32, 64, 64], P(('grp', 'ep'), 'tp'), parts along dimension 0, may hold values from -0.6 to 0.6
- head_decay_rate: float32 [32], P('tp'), may hold values from 0.05 to 4
- extra_log_decay: float32 [1024, 32], P(('grp', 'ep'), 'tp'), parts along dimension 0, may hold values from -0.7 to 0
- head_skip_weight: float32 [32], P('tp'), may hold values from 0.1 to 1.9
- output_matrix: bfloat16 [2048, 2048], P('tp'), may hold values from -0.125 to 0.125
- expert_norm_scale: bfloat16 [2048], replicated, may hold values from 0.099609375 to 1.8984375
- token_expert_index: int32 [1024, 6], P(('grp', 'ep')), parts along dimension 0, may hold values from 0 to 63, all different within a row; in each aligned block of 8 rows (0 to 7, 8 to 15, ...) at most 2 rows name the same one
- token_expert_weight: float32 [1024, 6], P(('grp', 'ep')), parts along dimension 0, may hold values from 0.2 to 1
- expert_gate_weight: bfloat16 [64, 2048, 704], P('ep', None, 'tp'), may hold values from -0.125 to 0.125
- expert_up_weight: bfloat16 [64, 2048, 704], P('ep', None, 'tp'), may hold values from -0.125 to 0.125
- expert_down_weight: bfloat16 [64, 704, 2048], P('ep', 'tp'), may hold values from -0.21875 to 0.21875
Outputs:
- layer_out: bfloat16 [1024, 2048], P(('grp', 'ep'), 'tp'), parts along dimension 0
- new_state: float32 [1024, 32, 64, 64], P(('grp', 'ep'), 'tp'), parts along dimension 0
- new_hist: bfloat16 [1024, 3, 2048], P(('grp', 'ep'), None, 'tp'), parts along dimension 0
The draws below stay inside these ranges and needn't reach their ends.
There are 2 independent parts, one for each index of `grp`. The reference program is written for one: setup_inputs(seed, part) draws one part's arguments, and reference() takes and returns one part's arrays. A program takes and returns all parts, laid end to end along the dimension named above; an argument that names none is the same for every part. Nothing has to cross between parts.
Inputs may be any that keep to these rules, and one draw needn't show every extreme that they name: `token_expert_index`: in the rows of one device (8 rows), no expert is named more than 2 times, and one expert is named exactly 2 times in some blocks; a token names 6 different experts.
All inputs are finite; a program needn't handle non-finite values.
Results may differ from the reference program's by a relative error of at most 0.015.
Values may be sent and summed in bfloat16 or wider, within the bound.
A program may use at most 64 MiB of HBM per device.

```python
import math
import jax
import jax.numpy as jnp
import numpy as np
from jax import lax

D = 2048
MIXER_HEADS = 32
HEAD_DIM = 64
GROUPS = 4
STATE_DIM = 64
TAPS = 4
EXP_FF = 704
TOPK = 6
SEQ_DEV = 8
SEQUENCE_COUNT = 512
EXPERTS = 64
CAP = 2
INNER = 2048
N_TP = 2


def block_scale(rng, extent, split, least, largest):
    loudness, own = 1.0, jax.random.fold_in(rng, 6)
    for axis_at, shards_of in split:
        draws = jnp.exp(jax.random.uniform(jax.random.fold_in(own, axis_at), (shards_of,), jnp.float32, least / len(split), largest / len(split)))
        loudness = loudness * jnp.repeat(draws, extent[axis_at] // shards_of).reshape([-1 if axis == axis_at else 1 for axis in range(len(extent))])
    return loudness


def assign_block(key, own, number, rows, number_of, top, limit, skew):
    sequence = jax.random.permutation(key, number_of)
    heavy_load, ordinary = shares(number_of, rows * top, limit, skew, True), shares(number_of, rows * top, limit, skew, False)
    places = jnp.arange(number_of)

    def named(sizes, rotation):
        used = int((sizes > 0).sum())
        fixed = max(1, used // 4)
        moved = fixed + (places - fixed + rotation * (used - fixed)) % max(1, number_of - fixed)
        return jnp.zeros((number_of,), jnp.int32).at[sequence[jnp.where(places < fixed, places, moved)]].set(jnp.asarray(sizes, jnp.int32))

    sizes = jnp.where(number % 4 == 0, named(heavy_load, number // 4), named(ordinary, number - number // 4 - 1))
    mixed = jax.random.permutation(jax.random.fold_in(own, 3), number_of)
    giver, taker = mixed[0:number_of // 2 * 2:2], mixed[1:number_of // 2 * 2:2]
    slack = jnp.minimum(sizes[giver] - 1, limit - sizes[taker]) // 2
    slack = jnp.where((giver == sequence[0]) | (taker == sequence[0]) | (sizes[taker] == 0), 0, jnp.maximum(slack, 0))
    moved = jax.random.randint(jax.random.fold_in(own, 4), (number_of // 2,), 0, 1 << 20) % (slack + 1)
    sizes = sizes.at[giver].add(-moved).at[taker].add(moved)
    items = jnp.searchsorted(jnp.cumsum(sizes), jnp.arange(rows * top), side="right").astype(jnp.int32)
    grid = items.reshape(top, rows).T
    grid = grid[jax.random.permutation(jax.random.fold_in(own, 1), rows)]
    rotation = jax.random.randint(jax.random.fold_in(own, 2), (rows, 1), 0, top)
    return jnp.take_along_axis(grid, (jnp.arange(top)[None, :] + rotation) % top, axis=1)


def shares(amount, total, reach, slope, full):
    portions = [(1 << 20) // math.isqrt(grade ** slope) + 1 for grade in range(1, amount + 1)]
    largest = reach if full else min(reach, max(-(-total // amount), total * portions[0] // sum(portions)))
    least = 1 if total - largest >= amount - 1 else 0
    counts, spare = [largest] + [least] * (amount - 1), total - largest - least * (amount - 1)
    while spare > 0:
        movable = [i for i in range(1, amount) if counts[i] < largest] or [i for i in range(1, amount) if counts[i] < reach]
        whole, left = sum([portions[i] for i in movable]), spare
        for i in movable:
            addition = min(reach - counts[i], max(1, left * portions[i] // whole), spare)
            counts[i] = counts[i] + addition
            spare = spare - addition
    return np.array(counts)


def bell_draw(key, extent, spread, bound, split=(), dtype=jnp.bfloat16):
    gain = block_scale(key, extent, split, -0.22, 0.18) if split else 1.0
    values = jax.random.normal(key, extent, jnp.float32) * spread * gain
    return jnp.minimum(jnp.maximum(values, -bound), bound).astype(dtype)


def setup_inputs(seed: int = 0, part: int = 0) -> dict:
    streams_of = jax.random.split(jax.random.key(seed), 20)
    part_keys = jax.random.split(jax.random.fold_in(streams_of[19], part), 20)
    hidden = bell_draw(part_keys[0], (SEQUENCE_COUNT, D), 1.0, 6.0, ((0, 64), (1, 2)))
    head_input_projected = bell_draw(part_keys[1], (SEQUENCE_COUNT, INNER), 1.0, 6.0, ((0, 64), (1, 2)))
    output_gate_projected = bell_draw(part_keys[2], (SEQUENCE_COUNT, INNER), 1.0, 6.0, ((0, 64), (1, 2)))
    input_map_projected = bell_draw(part_keys[3], (SEQUENCE_COUNT, GROUPS * STATE_DIM), 0.1, 0.59765625, ((0, 64), (1, 2)))
    output_map_projected = bell_draw(part_keys[4], (SEQUENCE_COUNT, GROUPS * STATE_DIM), 1.0, 6.0, ((0, 64), (1, 2)))
    raw_step_size = bell_draw(part_keys[5], (SEQUENCE_COUNT, MIXER_HEADS), 1.0, 5.0, ((0, 64), (1, 2)))
    convolution_history = bell_draw(part_keys[6], (SEQUENCE_COUNT, TAPS - 1, INNER), 1.0, 6.0, ((0, 64), (2, 2)))
    convolution_kernel = bell_draw(streams_of[7], (TAPS, INNER), TAPS ** -0.5, 3.0, ((1, 2),))
    recurrent_state_matrix = bell_draw(part_keys[8], (SEQUENCE_COUNT, MIXER_HEADS, HEAD_DIM, STATE_DIM), 0.1, 0.6, ((0, 64), (1, 2)), jnp.float32)
    head_decay_rate = jnp.clip(jnp.exp(math.log(4.0) - 4.3820266 * jax.random.uniform(streams_of[9], (MIXER_HEADS,), jnp.float32) ** block_scale(streams_of[9], (MIXER_HEADS,), ((0, 2),), -0.2, 0.2)), 0.05, 4.0)
    extra_log_decay = jnp.clip(-0.7 + 0.7 * jax.random.uniform(part_keys[10], (SEQUENCE_COUNT, MIXER_HEADS), jnp.float32) ** block_scale(part_keys[10], (SEQUENCE_COUNT, MIXER_HEADS), ((0, 64), (1, 2)), -0.2, 0.2), -0.7, 0.0)
    head_skip_weight = jnp.clip(1.0 + 0.18 * jax.random.normal(streams_of[11], (MIXER_HEADS,), jnp.float32), 0.1, 1.9)
    output_matrix = bell_draw(streams_of[12], (INNER, D), INNER ** -0.5, 0.125, ((0, 2),))
    expert_norm_scale = jnp.clip(1.0 + 0.18 * jax.random.normal(streams_of[13], (D,), jnp.float32), 0.099609375, 1.8984375).astype(jnp.bfloat16)
    token_expert_index_keys = jax.random.split(jax.random.fold_in(part_keys[14], 1), SEQUENCE_COUNT // SEQ_DEV)
    token_expert_index_turns = jax.random.permutation(jax.random.fold_in(part_keys[14], 3), SEQUENCE_COUNT // SEQ_DEV)
    token_expert_index = jax.vmap(lambda own, number: assign_block(jax.random.fold_in(part_keys[14], 2), own, number, SEQ_DEV, EXPERTS, TOPK, CAP, 2))(token_expert_index_keys, token_expert_index_turns).reshape((SEQUENCE_COUNT, TOPK))
    token_expert_weight = jnp.clip(0.2 + 0.8 * jax.random.uniform(part_keys[15], (SEQUENCE_COUNT, TOPK), jnp.float32) ** block_scale(part_keys[15], (SEQUENCE_COUNT, TOPK), ((0, 64),), -0.2, 0.2), 0.2, 1.0)
    expert_gate_weight = bell_draw(streams_of[16], (EXPERTS, D, EXP_FF), D ** -0.5, 0.125, ((0, 64), (2, 2)))
    expert_up_weight = bell_draw(streams_of[17], (EXPERTS, D, EXP_FF), D ** -0.5, 0.125, ((0, 64), (2, 2)))
    expert_down_weight = bell_draw(streams_of[18], (EXPERTS, EXP_FF, D), EXP_FF ** -0.5, 0.21875, ((0, 64), (1, 2)))
    return dict(hidden=hidden, head_input_projected=head_input_projected, output_gate_projected=output_gate_projected, input_map_projected=input_map_projected, output_map_projected=output_map_projected, raw_step_size=raw_step_size, convolution_history=convolution_history, convolution_kernel=convolution_kernel, recurrent_state_matrix=recurrent_state_matrix, head_decay_rate=head_decay_rate, extra_log_decay=extra_log_decay, head_skip_weight=head_skip_weight, output_matrix=output_matrix, expert_norm_scale=expert_norm_scale, token_expert_index=token_expert_index, token_expert_weight=token_expert_weight, expert_gate_weight=expert_gate_weight, expert_up_weight=expert_up_weight, expert_down_weight=expert_down_weight)


EPSILON = 1e-06

def reference(hidden, head_input_projected, output_gate_projected, input_map_projected, output_map_projected, raw_step_size, convolution_history, convolution_kernel, recurrent_state_matrix, head_decay_rate, extra_log_decay, head_skip_weight, output_matrix, expert_norm_scale, token_expert_index, token_expert_weight, expert_gate_weight, expert_up_weight, expert_down_weight):
    seq_total = hidden.shape[0]
    window = jnp.concatenate([convolution_history, head_input_projected[:, None, :]], axis=1)
    new_hist = window[:, 1:]
    conv = jax.nn.silu(lax.optimization_barrier(jnp.sum(window.astype(jnp.float32) * convolution_kernel.astype(jnp.float32)[None], axis=1)))
    discrete_update = jax.nn.softplus(raw_step_size.astype(jnp.float32))
    decay_factor = jnp.exp(-head_decay_rate[None, :] * discrete_update + extra_log_decay)
    per_group = MIXER_HEADS // GROUPS
    heads_in = conv.reshape(seq_total, MIXER_HEADS, HEAD_DIM)
    b_heads = jnp.repeat(input_map_projected.astype(jnp.float32).reshape(seq_total, GROUPS, STATE_DIM), per_group, axis=1)
    c_heads = jnp.repeat(output_map_projected.astype(jnp.float32).reshape(seq_total, GROUPS, STATE_DIM), per_group, axis=1)
    new_state = decay_factor[:, :, None, None] * recurrent_state_matrix + (discrete_update[:, :, None] * heads_in)[:, :, :, None] * b_heads[:, :, None, :]
    readout = jnp.einsum('shpn,shn->shp', new_state, c_heads) + head_skip_weight[None, :, None] * heads_in
    gated = (readout.reshape(seq_total, INNER) * jax.nn.silu(output_gate_projected.astype(jnp.float32))).astype(jnp.bfloat16)
    half_inner = INNER // N_TP
    mixed = jnp.zeros((seq_total, D), jnp.float32)
    for index in range(N_TP):
        part_mix = jnp.dot(gated[:, index * half_inner:(index + 1) * half_inner], output_matrix[index * half_inner:(index + 1) * half_inner], preferred_element_type=jnp.float32).astype(jnp.bfloat16)
        mixed = mixed + lax.optimization_barrier(part_mix).astype(jnp.float32)
    resid = (hidden.astype(jnp.float32) + mixed).astype(jnp.bfloat16)
    values = resid.astype(jnp.float32)
    inv_rms = lax.rsqrt(lax.optimization_barrier(jnp.mean(values * values, axis=-1, keepdims=True)) + EPSILON)
    normed = (values * expert_norm_scale.astype(jnp.float32)).astype(jnp.bfloat16)
    half_ff = EXP_FF // N_TP

    def one_token(inputs):
        row, scale, experts, weights = inputs
        total = jnp.zeros((D,), jnp.float32)
        for slot in range(TOPK):
            which = experts[slot]
            pre = scale * jnp.dot(row[None], expert_gate_weight[which], preferred_element_type=jnp.float32)
            lin = scale * jnp.dot(row[None], expert_up_weight[which], preferred_element_type=jnp.float32)
            act = (jax.nn.silu(pre) * lin).astype(jnp.bfloat16)
            down = expert_down_weight[which]
            summed = jnp.zeros((1, D), jnp.float32)
            for index in range(N_TP):
                part_out = jnp.dot(act[:, index * half_ff:(index + 1) * half_ff], down[index * half_ff:(index + 1) * half_ff], preferred_element_type=jnp.float32).astype(jnp.bfloat16)
                summed = summed + lax.optimization_barrier(part_out).astype(jnp.float32)
            result = summed.astype(jnp.bfloat16)
            total = total + weights[slot] * result[0].astype(jnp.float32)
        return total
    routed = lax.map(one_token, (normed, inv_rms[:, 0], token_expert_index, token_expert_weight))
    layer_out = (values + routed).astype(jnp.bfloat16)
    return (layer_out, new_state, new_hist)
```

```python
import functools

import jax
import jax.numpy as jnp
from jax import lax
from jax.experimental import pallas as pl
from jax.experimental.pallas import tpu as pltpu
from jax.sharding import PartitionSpec as P

MESH = pl.DeviceIdType.MESH
F32 = jnp.float32
BF16 = jnp.bfloat16

STATE_DIM = 64
TOPK = 6
CAP = 2
EPSILON = 1e-06
X_SIDE = 4
REACH = 4
LANES = 128
HIGH = lax.Precision.HIGHEST


def iota(shape, dim):
    return lax.broadcasted_iota(jnp.int32, shape, dim)


def silu(v):
    return v / (1.0 + jnp.exp(-v))


def softplus(v):
    return jnp.maximum(v, 0.0) + jnp.log1p(jnp.exp(-jnp.abs(v)))


def mixer_kernel(
    head_in, gate, b_map, c_map, raw_step, hist, taps, state, rate, extra, skip,
    new_state, new_hist, gated,
    conv_s, decay_s, u_t, y_s,
):
    step_at = pl.program_id(0)
    seqs, inner = head_in.shape
    heads = raw_step.shape[1]
    width = inner // heads
    groups = b_map.shape[1] // STATE_DIM
    per_group = heads // groups
    lanes_of = (iota((heads, inner), 1) // width == iota((heads, inner), 0)).astype(F32)

    @pl.when(step_at == 0)
    def _():
        x = head_in[...]
        for i in range(2):
            new_hist[i] = hist[i + 1]
        new_hist[2] = x
        kern = taps[...].astype(F32)
        total = x.astype(F32) * kern[3:4]
        for i in range(3):
            total = total + hist[i].astype(F32) * kern[i : i + 1]
        conv = silu(total)
        conv_s[...] = conv
        dt = softplus(raw_step[...].astype(F32))
        col = iota((seqs, heads), 1)
        rates = jnp.zeros((seqs, heads), F32)
        for h in range(heads):
            rates = jnp.where(col == h, rate[h], rates)
        decay_s[...] = jnp.exp(-rates * dt + extra[...])
        u = conv * jnp.dot(dt, lanes_of, precision=HIGH, preferred_element_type=F32)
        u_hi = u.astype(BF16).astype(F32)
        u_t[...] = jnp.concatenate([u_hi, u - u_hi], axis=0).T.astype(BF16)
        y_s[...] = jnp.zeros_like(y_s)

    row = iota((2 * seqs, STATE_DIM), 0)
    row_c = iota((seqs, STATE_DIM), 0)
    b_all = b_map[...]
    c_all = c_map[...]
    for g in range(groups):
        cols = slice(g * STATE_DIM, (g + 1) * STATE_DIM)
        b_g = jnp.concatenate([b_all[:, cols].astype(F32)] * 2, axis=0)
        b_g = jnp.where(row % seqs == step_at, b_g, 0.0).astype(BF16)
        c_g = jnp.where(row_c == step_at, c_all[:, cols].astype(F32), 0.0).astype(BF16)
        chans = per_group * width
        outer = jnp.dot(u_t[g * chans : (g + 1) * chans, :], b_g, preferred_element_type=F32)
        for j in range(per_group):
            h = g * per_group + j
            d = decay_s[pl.ds(step_at, 1), h : h + 1]
            new = d * state[0, h] + outer[j * width : (j + 1) * width]
            new_state[0, h] = new
        fresh = new_state[0, g * per_group : (g + 1) * per_group].reshape(chans, STATE_DIM)
        y_s[:, g * chans : (g + 1) * chans] += lax.dot_general(
            c_g, fresh.astype(BF16), (((1,), (1,)), ((), ())), preferred_element_type=F32
        )

    @pl.when(step_at == pl.num_programs(0) - 1)
    def _():
        col = iota((seqs, inner), 1) // width
        skips = jnp.zeros((seqs, inner), F32)
        for h in range(heads):
            skips = jnp.where(col == h, skip[h], skips)
        readout = y_s[...] + skips * conv_s[...]
        gated[...] = (readout * silu(gate[...].astype(F32))).astype(BF16)


def mixer(head_in, gate, b_map, c_map, raw_step, hist, taps, state, rate, extra, skip):
    seqs, inner = head_in.shape
    heads, width = state.shape[1:3]

    def whole(a):
        return pl.BlockSpec(a.shape, lambda i: (0,) * a.ndim)

    smem = pl.BlockSpec(memory_space=pltpu.SMEM)
    one = pl.BlockSpec((1,) + state.shape[1:], lambda i: (i, 0, 0, 0))
    return pl.pallas_call(
        mixer_kernel,
        name="mixer",
        grid=(seqs,),
        in_specs=[whole(head_in), whole(gate), whole(b_map), whole(c_map), whole(raw_step), whole(hist), whole(taps),
                  one, smem, whole(extra), smem],
        out_specs=[one, whole(hist), whole(head_in)],
        out_shape=[
            jax.ShapeDtypeStruct(state.shape, F32),
            jax.ShapeDtypeStruct(hist.shape, BF16),
            jax.ShapeDtypeStruct(head_in.shape, BF16),
        ],
        scratch_shapes=[
            pltpu.VMEM((seqs, inner), F32),
            pltpu.VMEM((seqs, heads), F32),
            pltpu.VMEM((inner, 2 * seqs), BF16),
            pltpu.VMEM((seqs, inner), F32),
        ],
        compiler_params=pltpu.CompilerParams(dimension_semantics=("arbitrary",)),
    )(head_in, gate, b_map, c_map, raw_step, hist, taps, state, rate, extra, skip)


def expert_kernel(
    gated, hidden, wout_h, norm, chosen, weights, wg_h, wu_h, wd_h,
    out,
    wout, wg, wu, wd, tp_tx, tp_rx, tokens, pick_tx, pick_rx, pick_other, down_tx, down_rx, back_tx, back_rx,
    sums, sums_bf, relay_rx, relay_tx, last_rx,
    w_sem, tp_s, tp_r, z_s, z_r, x_s, x_r, o_s, o_r, d_s, d_r, b_s, b_r, h_s, h_r,
):
    seqs, half = hidden.shape
    nz = tokens.shape[0]
    slots = nz * CAP
    rows = X_SIDE * slots
    me, core = lax.axis_index("ep"), lax.axis_index("tp")
    z, x = me // X_SIDE, me % X_SIDE
    other = 1 - core

    def along_z(d):
        return {"ep": ((z + d + nz) % nz) * X_SIDE + x}

    def along_x(d):
        return {"ep": z * X_SIDE + (x + d) % X_SIDE}

    partner = {"tp": other}
    mine_cols = pl.ds(pl.multiple_of(core * half, half), half)
    other_cols = pl.ds(pl.multiple_of(other * half, half), half)

    loads = [
        pltpu.make_async_copy(wout_h, wout, w_sem.at[0]),
        pltpu.make_async_copy(wg_h.at[0], wg, w_sem.at[1]),
        pltpu.make_async_copy(wu_h.at[0], wu, w_sem.at[2]),
        pltpu.make_async_copy(wd_h.at[0], wd, w_sem.at[3]),
    ]
    for load in loads:
        load.start()

    barrier = pltpu.get_barrier_semaphore()
    z_steps = [s * d for d in range(REACH, 0, -1) for s in (1, -1)]
    peers = [along_z(d) for d in z_steps] + [along_x(d) for d in range(1, X_SIDE)] + [partner]
    for peer in peers:
        pl.semaphore_signal(barrier, inc=1, device_id=peer, device_id_type=MESH)

    idx = chosen[...]
    wts = weights[...]
    lane = iota((seqs, LANES), 1)
    named = jnp.zeros((seqs, LANES), F32)
    for i in range(TOPK):
        named = named + (lane == idx[:, i : i + 1]).astype(F32)
    before = (iota((seqs, seqs), 1) < iota((seqs, seqs), 0)).astype(BF16)
    rank = jnp.dot(before, named.astype(BF16), preferred_element_type=F32)
    extra = jnp.zeros((seqs, LANES), F32)
    for i in range(TOPK):
        expert = idx[:, i : i + 1]
        place = jnp.sum(jnp.where(lane == expert, rank, 0.0), axis=1, keepdims=True)
        slot = expert.astype(F32) * CAP + place
        w = wts[:, i : i + 1]
        w_hi = w.astype(BF16).astype(F32)
        extra = jnp.where(lane == i, slot, extra)
        extra = jnp.where(lane == TOPK + i, w_hi, extra)
        extra = jnp.where(lane == 2 * TOPK + i, w - w_hi, extra)
    tokens[z, :, half:] = extra.astype(BF16)

    def remote(src, dst, send, recv, peer):
        return pltpu.make_async_remote_copy(
            src_ref=src, dst_ref=dst, send_sem=send, recv_sem=recv, device_id=peer, device_id_type=MESH
        )

    loads[0].wait()
    tp_tx[...] = jnp.dot(gated[...], wout[:, other_cols], preferred_element_type=F32).astype(BF16)
    own_mix = jnp.dot(gated[...], wout[:, mine_cols], preferred_element_type=F32).astype(BF16)
    pl.semaphore_wait(barrier, len(peers))
    swap = remote(tp_tx, tp_rx, tp_s, tp_r, partner)
    swap.start()
    base = hidden[...].astype(F32)
    swap.wait()
    mixed = own_mix.astype(F32) + tp_rx[...].astype(F32)
    resid = (base + mixed).astype(BF16)
    tokens[z, :, :half] = resid

    def block(origin):
        return tokens.at[(origin + nz) % nz]

    copies, arrivals = [], []
    for d in z_steps:
        q = len(copies)
        copies.append(remote(block(z), block(z), z_s.at[q], z_r.at[q], along_z(d)))
        arrivals.append(remote(block(z - d), block(z - d), z_s.at[q], z_r.at[q], along_z(d)))
        copies[q].start()
    far_up, far_down = nz // 2 - REACH, nz - 1 - nz // 2 - REACH
    for sign, count in ((1, far_up), (-1, far_down)):
        arrivals[0 if sign == 1 else 1].wait_recv()
        for hop in range(count, 0, -1):
            q = len(copies)
            origin, there = z - sign * REACH, z - sign * (REACH + hop)
            copies.append(remote(block(origin), block(origin), z_s.at[q], z_r.at[q], along_z(sign * hop)))
            arrivals.append(remote(block(there), block(there), z_s.at[q], z_r.at[q], along_z(sign * hop)))
            copies[q].start()
    for q in range(2, len(copies)):
        arrivals[q].wait_recv()

    held = tokens[...].astype(F32).reshape(nz * seqs, half + LANES)
    info = held[:, half:]
    info = info + jnp.where(iota(info.shape, 1) < TOPK, 0.0, pltpu.roll(info, LANES - TOPK, 1))
    row_z = iota((nz * seqs, rows), 0) // seqs
    col = iota((nz * seqs, rows), 1)
    slot_of = ((z * X_SIDE + col // slots) * CAP + col % CAP).astype(F32)
    same_z = (col % slots) // CAP == row_z
    takes = jnp.zeros((nz * seqs, rows), F32)
    mixing = jnp.zeros((nz * seqs, rows), F32)
    for i in range(TOPK):
        hit = same_z & (info[:, i : i + 1] == slot_of)
        takes = jnp.where(hit, 1.0, takes)
        mixing = jnp.where(hit, info[:, TOPK + i : TOPK + i + 1], mixing)
    mix_hi = mixing.astype(BF16)
    mix_lo = (mixing - mix_hi.astype(F32)).astype(BF16)
    picked = jnp.dot(takes.T.astype(BF16), held[:, :half].astype(BF16), preferred_element_type=F32).astype(BF16)
    pick_tx[...] = picked.reshape(X_SIDE, slots, half)

    def at_x(ref, d):
        return ref.at[(x + d + X_SIDE) % X_SIDE]

    order = [2, 1, 3]
    sent = []
    for i, d in enumerate(order):
        sent.append(remote(at_x(pick_tx, d), pick_rx.at[x], x_s.at[i], x_r.at[i], along_x(d)))
        sent[i].start()
    pick_rx[x] = pick_tx[x]
    shared = [remote(pick_tx.at[x], pick_other.at[x], o_s.at[3], o_r.at[3], partner)]
    shared[0].start()
    for i in (1, 2, 0):
        d = order[i]
        got = at_x(pick_rx, -d)
        remote(got, got, x_s.at[i], x_r.at[i], along_x(d)).wait_recv()
        shared.append(remote(got, at_x(pick_other, -d), o_s.at[i], o_r.at[i], partner))
        shared[-1].start()

    def project(values, cols):
        f = values[...].reshape(rows, half).astype(F32)
        scaled = (f * norm[0:1, cols].astype(F32)).astype(BF16)
        dims = (((1,), (1,)), ((), ()))
        g = lax.dot_general(scaled, wg[:, cols], dims, preferred_element_type=F32)
        u = lax.dot_general(scaled, wu[:, cols], dims, preferred_element_type=F32)
        return g, u, jnp.sum(f * f, axis=1, keepdims=True)

    for load in loads[1:]:
        load.wait()
    g0, u0, s0 = project(pick_rx, mine_cols)
    for copy in shared:
        copy.wait_recv()
    g1, u1, s1 = project(pick_other, other_cols)
    inv = lax.rsqrt((s0 + s1) / (2 * half) + EPSILON)
    act = (silu(inv * (g0 + g1)) * (inv * (u0 + u1))).astype(BF16)
    down_tx[...] = jnp.dot(act, wd[:, other_cols], preferred_element_type=F32).astype(BF16)
    trade = remote(down_tx, down_rx, d_s, d_r, partner)
    trade.start()
    own_down = jnp.dot(act, wd[:, mine_cols], preferred_element_type=F32).astype(BF16)
    trade.wait_recv()
    result = (own_down.astype(F32) + down_rx[...].astype(F32)).astype(BF16)
    back_tx[...] = result.reshape(X_SIDE, slots, half)

    returned = []
    for i, d in enumerate(order):
        returned.append(remote(at_x(back_tx, d), back_rx.at[x], b_s.at[i], b_r.at[i], along_x(d)))
        returned[i].start()
    back_rx[x] = back_tx[x]
    for i, d in enumerate(order):
        got = at_x(back_rx, -d)
        remote(got, got, b_s.at[i], b_r.at[i], along_x(d)).wait_recv()
    rows_back = back_rx[...].reshape(rows, half)
    part = jnp.dot(mix_hi, rows_back, preferred_element_type=F32) + jnp.dot(mix_lo, rows_back, preferred_element_type=F32)
    part = part.reshape(nz, seqs, half)
    sums[...] = part
    sums_bf[...] = part.astype(BF16)

    def at_z(ref, d):
        return ref.at[(z + d + nz) % nz]

    parts = []

    def send(src, dst, peer):
        q = len(parts)
        parts.append(remote(src, dst, h_s.at[q], h_r.at[q], peer))
        parts[q].start()

    for sign, count, first in ((1, far_up, 0), (-1, far_down, far_up)):
        for hop in range(count, 0, -1):
            send(at_z(sums_bf, -sign * (REACH + hop)), relay_rx.at[first + hop - 1], along_z(-sign * hop))
    near = [d for d in z_steps if abs(d) < REACH]
    for i, d in enumerate(near):
        send(at_z(sums_bf, -d), last_rx.at[i], along_z(-d))
    for n, (sign, count, first) in enumerate(((1, far_up, 0), (-1, far_down, far_up))):
        total = at_z(sums, -sign * REACH)[...]
        for hop in range(count, 0, -1):
            parts[first + count - hop].wait_recv()
            total = total + relay_rx[first + hop - 1].astype(F32)
        relay_tx[n] = total.astype(BF16)
        send(relay_tx.at[n], last_rx.at[len(near) + n], along_z(-sign * REACH))
    total = resid.astype(F32) + at_z(sums, 0)[...]
    for i in range(len(near) + 2):
        parts[far_up + far_down + i].wait_recv()
        total = total + last_rx[i].astype(F32)
    out[...] = total.astype(BF16)

    swap_done = [*copies, *sent, *shared, trade, *returned, *parts]
    for copy in swap_done:
        copy.wait_send()


def experts(ep, gated, hidden, wout, norm, chosen, weights, wg, wu, wd):
    seqs, half = hidden.shape
    nz = ep // X_SIDE
    slots = nz * CAP
    rows = X_SIDE * slots
    vmem = pl.BlockSpec(memory_space=pltpu.VMEM)
    hbm = pl.BlockSpec(memory_space=pl.ANY)
    dma = pltpu.SemaphoreType.DMA
    one = dma(())
    far = nz - 1 - 2 * REACH
    return pl.pallas_call(
        expert_kernel,
        name="experts",
        in_specs=[vmem, vmem, hbm, vmem, vmem, vmem, hbm, hbm, hbm],
        out_specs=vmem,
        out_shape=jax.ShapeDtypeStruct(hidden.shape, BF16),
        scratch_shapes=[
            pltpu.VMEM(wout.shape, BF16),
            pltpu.VMEM(wg.shape[1:], BF16),
            pltpu.VMEM(wu.shape[1:], BF16),
            pltpu.VMEM(wd.shape[1:], BF16),
            pltpu.VMEM((seqs, half), BF16),
            pltpu.VMEM((seqs, half), BF16),
            pltpu.VMEM((nz, seqs, half + LANES), BF16),
            pltpu.VMEM((X_SIDE, slots, half), BF16),
            pltpu.VMEM((X_SIDE, slots, half), BF16),
            pltpu.VMEM((X_SIDE, slots, half), BF16),
            pltpu.VMEM((rows, half), BF16),
            pltpu.VMEM((rows, half), BF16),
            pltpu.VMEM((X_SIDE, slots, half), BF16),
            pltpu.VMEM((X_SIDE, slots, half), BF16),
            pltpu.VMEM((nz, seqs, half), F32),
            pltpu.VMEM((nz, seqs, half), BF16),
            pltpu.VMEM((far, seqs, half), BF16),
            pltpu.VMEM((2, seqs, half), BF16),
            pltpu.VMEM((2 * REACH, seqs, half), BF16),
            dma((4,)), one, one, dma((nz - 1,)), dma((nz - 1,)), dma((3,)), dma((3,)), dma((4,)), dma((4,)),
            one, one, dma((3,)), dma((3,)), dma((nz - 1,)), dma((nz - 1,)),
        ],
        compiler_params=pltpu.CompilerParams(
            collective_id=0, has_side_effects=True, vmem_limit_bytes=40 * 1024 * 1024
        ),
    )(gated, hidden, wout, norm, chosen, weights, wg, wu, wd)


def on_device(
    ep,
    hidden,
    head_input_projected,
    output_gate_projected,
    input_map_projected,
    output_map_projected,
    raw_step_size,
    convolution_history,
    convolution_kernel,
    recurrent_state_matrix,
    head_decay_rate,
    extra_log_decay,
    head_skip_weight,
    output_matrix,
    expert_norm_scale,
    token_expert_index,
    token_expert_weight,
    expert_gate_weight,
    expert_up_weight,
    expert_down_weight,
):
    new_state, new_hist, gated = mixer(
        head_input_projected,
        output_gate_projected,
        input_map_projected,
        output_map_projected,
        raw_step_size,
        jnp.swapaxes(convolution_history, 0, 1),
        convolution_kernel,
        recurrent_state_matrix,
        head_decay_rate,
        extra_log_decay,
        head_skip_weight,
    )
    layer_out = experts(
        ep,
        gated,
        hidden,
        output_matrix,
        expert_norm_scale[None, :],
        token_expert_index,
        token_expert_weight,
        jnp.swapaxes(expert_gate_weight, 1, 2),
        jnp.swapaxes(expert_up_weight, 1, 2),
        expert_down_weight,
    )
    return (layer_out, new_state, jnp.swapaxes(new_hist, 0, 1))


def solution(mesh):
    in_specs = (
        P(("grp", "ep"), "tp"),
        P(("grp", "ep"), "tp"),
        P(("grp", "ep"), "tp"),
        P(("grp", "ep"), "tp"),
        P(("grp", "ep"), "tp"),
        P(("grp", "ep"), "tp"),
        P(("grp", "ep"), None, "tp"),
        P(None, "tp"),
        P(("grp", "ep"), "tp", None, None),
        P("tp"),
        P(("grp", "ep"), "tp"),
        P("tp"),
        P("tp", None),
        P(),
        P(("grp", "ep"), None),
        P(("grp", "ep"), None),
        P("ep", None, "tp"),
        P("ep", None, "tp"),
        P("ep", "tp", None),
    )
    out_specs = (
        P(("grp", "ep"), "tp"),
        P(("grp", "ep"), "tp", None, None),
        P(("grp", "ep"), None, "tp"),
    )
    return jax.shard_map(
        functools.partial(on_device, mesh.shape["ep"]),
        mesh=mesh,
        in_specs=in_specs,
        out_specs=out_specs,
        check_vma=False,
    )
```

```python
import functools

import jax
import jax.numpy as jnp
from jax import lax
from jax.experimental import pallas as pl
from jax.experimental.pallas import tpu as pltpu
from jax.sharding import PartitionSpec as P

MESH = pl.DeviceIdType.MESH
F32 = jnp.float32
BF16 = jnp.bfloat16

STATE_DIM = 64
TOPK = 6
CAP = 2
EPSILON = 1e-06
X_SIDE = 4
FIRST = [(0, (5, -5, 2, -2, 1, -1))]
FAN = [(5, (3, 2, -2, 1, -1)), (11, (-2, 2, -1, 1))]
LANES = 128
HIGH = lax.Precision.HIGHEST
VMEM_BYTES = 28 * 1024 * 1024


def iota(shape, dim):
    return lax.broadcasted_iota(jnp.int32, shape, dim)


def silu(v):
    return v / (1.0 + jnp.exp(-v))


def softplus(v):
    return jnp.maximum(v, 0.0) + jnp.log1p(jnp.exp(-jnp.abs(v)))


def layer_kernel(
    hidden_h, head_in_h, gate_h, b_map_h, c_map_h, raw_step_h, hist_h, taps_h, state_h, rate_h, extra_h, skip_h, wout_h,
    norm_h, chosen_h, weights_h, wg_h, wu_h, wd_h,
    out, new_state, new_hist,
    hidden, head_in, gate, b_map, c_map, raw_step, hist, taps, state, rate, extra_decay, skip, wout,
    norm, chosen, weights, wg, wu, wd,
    tp_tx, tp_rx, tokens, pick_tx, pick_rx, pick_other, down_tx, down_rx, back_tx, back_rx,
    sums, sums_bf, relay_rx, relay_tx, last_rx,
    in_sem, w_sem, tp_s, tp_r, z_s, z_r, x_s, x_r, o_s, o_r, d_s, d_r, b_s, b_r, h_s, h_r,
):
    seqs, half = hidden.shape
    nz = tokens.shape[0]
    slots = nz * CAP
    rows = X_SIDE * slots
    me, core = lax.axis_index("ep"), lax.axis_index("tp")
    z, x = me // X_SIDE, me % X_SIDE
    other = 1 - core

    def along_z(d):
        return {"ep": ((z + d + nz) % nz) * X_SIDE + x}

    def along_x(d):
        return {"ep": z * X_SIDE + (x + d) % X_SIDE}

    partner = {"tp": other}
    mine_cols = pl.ds(pl.multiple_of(core * half, half), half)
    other_cols = pl.ds(pl.multiple_of(other * half, half), half)

    barrier = pltpu.get_barrier_semaphore()
    steps = sorted({s * h for _, hops in FIRST + FAN for h in hops for s in (1, -1)})
    peers = [along_z(h) for h in steps] + [along_x(d) for d in range(1, X_SIDE)] + [partner]
    for peer in peers:
        pl.semaphore_signal(barrier, inc=1, device_id=peer, device_id_type=MESH)
    pairs = [(head_in_h, head_in), (hist_h, hist), (taps_h, taps), (raw_step_h, raw_step), (extra_h, extra_decay), (rate_h, rate),
             (skip_h, skip), (b_map_h, b_map), (c_map_h, c_map), (gate_h, gate), (hidden_h, hidden), (chosen_h, chosen),
             (weights_h, weights), (norm_h, norm)]
    small = [pltpu.make_async_copy(src, dst, in_sem.at[i]) for i, (src, dst) in enumerate(pairs)]
    for copy in small:
        copy.start()
    fetch = [pltpu.make_async_copy(state_h.at[s], state.at[s], in_sem.at[len(pairs) + s]) for s in range(seqs)]
    for copy in fetch:
        copy.start()
    get_wout = pltpu.make_async_copy(wout_h, wout, w_sem.at[0])
    loads = [pltpu.make_async_copy(src, dst, w_sem.at[1 + i])
             for i, (src, dst) in enumerate([(wg_h.at[0], wg), (wu_h.at[0], wu), (wd_h.at[0], wd)])]
    for copy in small:
        copy.wait()

    heads = raw_step.shape[1]
    width = half // heads
    groups = b_map.shape[1] // STATE_DIM
    per_group = heads // groups
    chans = per_group * width
    fresh_in = head_in[...]
    for i in range(2):
        new_hist[i] = hist[i + 1]
    new_hist[2] = fresh_in
    kern = taps[...].astype(F32)
    total = fresh_in.astype(F32) * kern[3:4]
    for i in range(3):
        total = total + hist[i].astype(F32) * kern[i : i + 1]
    conv = silu(total)
    dt = softplus(raw_step[...].astype(F32))
    col = iota((seqs, heads), 1)
    rates = jnp.zeros((seqs, heads), F32)
    for h in range(heads):
        rates = jnp.where(col == h, rate[h], rates)
    decay = jnp.exp(-rates * dt + extra_decay[...])
    lanes_of = (iota((heads, half), 1) // width == iota((heads, half), 0)).astype(F32)
    spread = jnp.dot(jnp.concatenate([dt, decay], axis=0), lanes_of, precision=HIGH, preferred_element_type=F32)
    u = conv * spread[:seqs]
    decays = spread[seqs:]
    col = iota((seqs, half), 1) // width
    skips = jnp.zeros((seqs, half), F32)
    for h in range(heads):
        skips = jnp.where(col == h, skip[h], skips)
    opened = silu(gate[...].astype(F32))
    b_all = b_map[...].astype(F32)
    c_all = c_map[...].astype(F32)

    row_c = iota((seqs, STATE_DIM), 0)
    read = []
    for g in range(groups):
        cols = slice(g * STATE_DIM, (g + 1) * STATE_DIM)
        read.append(u[:, g * chans : (g + 1) * chans] * jnp.sum(b_all[:, cols] * c_all[:, cols], axis=1, keepdims=True))
    seen = [jnp.zeros((seqs, chans), F32) for _ in range(groups)]
    for s in range(seqs):
        fetch[s].wait()
        if s == seqs // 2:
            get_wout.start()
        for g in range(groups):
            c_g = jnp.where(row_c == s, c_all[:, g * STATE_DIM : (g + 1) * STATE_DIM], 0.0).astype(BF16)
            held = state[s, g * per_group : (g + 1) * per_group].reshape(chans, STATE_DIM).astype(BF16)
            seen[g] = seen[g] + lax.dot_general(c_g, held, (((1,), (1,)), ((), ())), preferred_element_type=F32)
    for load in loads:
        load.start()
    readout = decays * jnp.concatenate(seen, axis=1) + jnp.concatenate(read, axis=1) + skips * conv
    gated = (readout * opened).astype(BF16)

    idx = chosen[...]
    wts = weights[...]
    lane = iota((seqs, LANES), 1)
    named = jnp.zeros((seqs, LANES), F32)
    for i in range(TOPK):
        named = named + (lane == idx[:, i : i + 1]).astype(F32)
    before = (iota((seqs, seqs), 1) < iota((seqs, seqs), 0)).astype(BF16)
    rank = jnp.dot(before, named.astype(BF16), preferred_element_type=F32)
    extra = jnp.zeros((seqs, LANES), F32)
    for i in range(TOPK):
        expert = idx[:, i : i + 1]
        place = jnp.sum(jnp.where(lane == expert, rank, 0.0), axis=1, keepdims=True)
        slot = expert.astype(F32) * CAP + place
        w = wts[:, i : i + 1]
        w_hi = w.astype(BF16).astype(F32)
        extra = jnp.where(lane == i, slot, extra)
        extra = jnp.where(lane == TOPK + i, w_hi, extra)
        extra = jnp.where(lane == 2 * TOPK + i, w - w_hi, extra)
    tokens[0, :, half:] = extra.astype(BF16)

    def remote(src, dst, send, recv, peer):
        return pltpu.make_async_remote_copy(
            src_ref=src, dst_ref=dst, send_sem=send, recv_sem=recv, device_id=peer, device_id_type=MESH
        )

    get_wout.wait()
    tp_tx[...] = jnp.dot(gated, wout[:, other_cols], preferred_element_type=F32).astype(BF16)
    pl.semaphore_wait(barrier, len(peers))
    swap = remote(tp_tx, tp_rx, tp_s, tp_r, partner)
    swap.start()
    own_mix = jnp.dot(gated, wout[:, mine_cols], preferred_element_type=F32).astype(BF16)
    base = hidden[...].astype(F32)
    swap.wait()
    mixed = own_mix.astype(F32) + tp_rx[...].astype(F32)
    resid = (base + mixed).astype(BF16)
    tokens[0, :, :half] = resid

    def update_states():
        u_hi = u.astype(BF16).astype(F32)
        u_t = jnp.concatenate([u_hi, u - u_hi], axis=0).T.astype(BF16)
        row = iota((2 * seqs, STATE_DIM), 0)
        for s in range(seqs):
            for g in range(groups):
                b_g = b_all[:, g * STATE_DIM : (g + 1) * STATE_DIM]
                b_g = jnp.where(row % seqs == s, jnp.concatenate([b_g, b_g], axis=0), 0.0).astype(BF16)
                outer = jnp.dot(u_t[g * chans : (g + 1) * chans], b_g, preferred_element_type=F32)
                for j in range(per_group):
                    h = g * per_group + j
                    new_state[s, h] = decay[s : s + 1, h : h + 1] * state[s, h] + outer[j * width : (j + 1) * width]

    copies, arrived = [], {}
    for origin, hops in FIRST + FAN:
        if origin == FAN[0][0]:
            update_states()
        if origin:
            arrived.pop(origin).wait_recv()
        for hop in hops:
            q = len(copies)
            lands = (origin + hop) % nz
            copies.append(remote(tokens.at[origin], tokens.at[lands], z_s.at[q], z_r.at[q], along_z(hop)))
            arrived[lands] = copies[q]
            copies[q].start()
    for copy in arrived.values():
        copy.wait_recv()

    held = tokens[...].astype(F32).reshape(nz * seqs, half + LANES)
    info = held[:, half:]
    info = info + jnp.where(iota(info.shape, 1) < TOPK, 0.0, pltpu.roll(info, LANES - TOPK, 1))
    row_z = iota((nz * seqs, rows), 0) // seqs
    col = iota((nz * seqs, rows), 1)
    slot_of = ((z * X_SIDE + col // slots) * CAP + col % CAP).astype(F32)
    same_z = (col % slots) // CAP == row_z
    takes = jnp.zeros((nz * seqs, rows), F32)
    mixing = jnp.zeros((nz * seqs, rows), F32)
    for i in range(TOPK):
        hit = same_z & (info[:, i : i + 1] == slot_of)
        takes = jnp.where(hit, 1.0, takes)
        mixing = jnp.where(hit, info[:, TOPK + i : TOPK + i + 1], mixing)
    mix_hi = mixing.astype(BF16)
    mix_lo = (mixing - mix_hi.astype(F32)).astype(BF16)
    picked = jnp.dot(takes.T.astype(BF16), held[:, :half].astype(BF16), preferred_element_type=F32).astype(BF16)
    pick_tx[...] = picked.reshape(X_SIDE, slots, half)

    def at_x(ref, d):
        return ref.at[(x + d + X_SIDE) % X_SIDE]

    order = [2, 1, 3]
    sent = []
    for i, d in enumerate(order):
        sent.append(remote(at_x(pick_tx, d), pick_rx.at[x], x_s.at[i], x_r.at[i], along_x(d)))
        sent[i].start()
    pick_rx[x] = pick_tx[x]
    shared = [remote(pick_tx.at[x], pick_other.at[x], o_s.at[3], o_r.at[3], partner)]
    shared[0].start()
    for i in (1, 2, 0):
        d = order[i]
        got = at_x(pick_rx, -d)
        remote(got, got, x_s.at[i], x_r.at[i], along_x(d)).wait_recv()
        shared.append(remote(got, at_x(pick_other, -d), o_s.at[i], o_r.at[i], partner))
        shared[-1].start()

    def project(values, cols):
        f = values[...].reshape(rows, half).astype(F32)
        scaled = (f * norm[cols].astype(F32)[None, :]).astype(BF16)
        dims = (((1,), (1,)), ((), ()))
        g = lax.dot_general(scaled, wg[:, cols], dims, preferred_element_type=F32)
        u = lax.dot_general(scaled, wu[:, cols], dims, preferred_element_type=F32)
        return g, u, jnp.sum(f * f, axis=1, keepdims=True)

    for load in loads:
        load.wait()
    g0, u0, s0 = project(pick_rx, mine_cols)
    for copy in shared:
        copy.wait_recv()
    g1, u1, s1 = project(pick_other, other_cols)
    inv = lax.rsqrt((s0 + s1) / (2 * half) + EPSILON)
    act = (silu(inv * (g0 + g1)) * (inv * (u0 + u1))).astype(BF16)
    down_tx[...] = jnp.dot(act, wd[:, other_cols], preferred_element_type=F32).astype(BF16)
    trade = remote(down_tx, down_rx, d_s, d_r, partner)
    trade.start()
    own_down = jnp.dot(act, wd[:, mine_cols], preferred_element_type=F32).astype(BF16)
    trade.wait_recv()
    result = (own_down.astype(F32) + down_rx[...].astype(F32)).astype(BF16)
    back_tx[...] = result.reshape(X_SIDE, slots, half)

    returned = []
    for i, d in enumerate(order):
        returned.append(remote(at_x(back_tx, d), back_rx.at[x], b_s.at[i], b_r.at[i], along_x(d)))
        returned[i].start()
    back_rx[x] = back_tx[x]
    for i, d in enumerate(order):
        got = at_x(back_rx, -d)
        remote(got, got, b_s.at[i], b_r.at[i], along_x(d)).wait_recv()
    rows_back = back_rx[...].reshape(rows, half)
    part = jnp.dot(mix_hi, rows_back, preferred_element_type=F32) + jnp.dot(mix_lo, rows_back, preferred_element_type=F32)
    part = part.reshape(nz, seqs, half)
    sums[...] = part
    sums_bf[...] = part.astype(BF16)

    parts = []

    def send(src, dst, hop):
        q = len(parts)
        parts.append(remote(src, dst, h_s.at[q], h_r.at[q], along_z(hop)))
        parts[q].start()
        return parts[q]

    gathered = {}
    n = 0
    for origin, hops in FAN:
        for hop in hops:
            gathered.setdefault(origin, []).append((send(sums_bf.at[(origin + hop) % nz], relay_rx.at[n], -hop), n))
            n += 1
    finals = []
    (_, first_hops), = FIRST
    for hop in first_hops[len(FAN):]:
        finals.append(send(sums_bf.at[hop % nz], last_rx.at[len(finals)], -hop))
    for i, (origin, _) in enumerate(FAN):
        total = sums[origin]
        for copy, at in gathered[origin]:
            copy.wait_recv()
            total = total + relay_rx[at].astype(F32)
        relay_tx[i] = total.astype(BF16)
        finals.append(send(relay_tx.at[i], last_rx.at[len(finals)], -first_hops[i]))
    total = resid.astype(F32) + sums[0]
    for i, copy in enumerate(finals):
        copy.wait_recv()
        total = total + last_rx[i].astype(F32)
    out[...] = total.astype(BF16)

    swap_done = [*copies, *sent, *shared, trade, *returned, *parts]
    for copy in swap_done:
        copy.wait_send()


def layer(ep, *args):
    hidden, head_in, gate, b_map, c_map, raw_step, hist, taps, state, rate, extra, skip, wout, norm, chosen, weights, wg, wu, wd = args
    seqs, half = hidden.shape
    nz = ep // X_SIDE
    slots = nz * CAP
    rows = X_SIDE * slots
    far = sum(len(hops) for _, hops in FAN)
    near = len(FIRST[0][1])
    vmem = pl.BlockSpec(memory_space=pltpu.VMEM)
    hbm = pl.BlockSpec(memory_space=pltpu.HBM)
    dma = pltpu.SemaphoreType.DMA
    one = dma(())

    def room(a):
        return pltpu.VMEM(a.shape, a.dtype)

    return pl.pallas_call(
        layer_kernel,
        name="layer",
        in_specs=[hbm] * len(args),
        out_specs=[vmem, vmem, vmem],
        out_shape=[
            pltpu.VMEM(hidden.shape, BF16),
            pltpu.VMEM(state.shape, F32),
            pltpu.VMEM(hist.shape, BF16),
        ],
        scratch_shapes=[
            *(pltpu.SMEM(a.shape, F32) if a is rate or a is skip else room(a) for a in args[:16]),
            *(pltpu.VMEM(a.shape[1:], BF16) for a in (wg, wu, wd)),
            room(hidden),
            room(hidden),
            pltpu.VMEM((nz, seqs, half + LANES), BF16),
            *(pltpu.VMEM((X_SIDE, slots, half), BF16) for _ in range(3)),
            *(pltpu.VMEM((rows, half), BF16) for _ in range(2)),
            *(pltpu.VMEM((X_SIDE, slots, half), BF16) for _ in range(2)),
            pltpu.VMEM((nz, seqs, half), F32),
            pltpu.VMEM((nz, seqs, half), BF16),
            pltpu.VMEM((far, seqs, half), BF16),
            pltpu.VMEM((2, seqs, half), BF16),
            pltpu.VMEM((near, seqs, half), BF16),
            dma((14 + seqs,)), dma((4,)), one, one, dma((nz - 1,)), dma((nz - 1,)), dma((3,)), dma((3,)), dma((4,)), dma((4,)),
            one, one, dma((3,)), dma((3,)), dma((nz - 1,)), dma((nz - 1,)),
        ],
        compiler_params=pltpu.CompilerParams(collective_id=0, has_side_effects=True, vmem_limit_bytes=VMEM_BYTES),
    )(*(pltpu.with_memory_space_constraint(a, pltpu.HBM) for a in args))


def store_kernel(*refs):
    count = (len(refs) - 1) // 2
    sem = refs[-1]
    copies = [pltpu.make_async_copy(refs[i], refs[count + i], sem.at[i]) for i in range(count)]
    for copy in copies:
        copy.start()
    for copy in copies:
        copy.wait()


def store(*values):
    return pl.pallas_call(
        store_kernel,
        name="store",
        in_specs=[pl.BlockSpec(memory_space=pltpu.VMEM)] * len(values),
        out_specs=[pl.BlockSpec(memory_space=pltpu.HBM)] * len(values),
        out_shape=[pltpu.HBM(v.shape, v.dtype) for v in values],
        scratch_shapes=[pltpu.SemaphoreType.DMA((len(values),))],
        compiler_params=pltpu.CompilerParams(vmem_limit_bytes=VMEM_BYTES),
    )(*(pltpu.with_memory_space_constraint(v, pltpu.VMEM) for v in values))


def on_device(
    ep,
    hidden,
    head_input_projected,
    output_gate_projected,
    input_map_projected,
    output_map_projected,
    raw_step_size,
    convolution_history,
    convolution_kernel,
    recurrent_state_matrix,
    head_decay_rate,
    extra_log_decay,
    head_skip_weight,
    output_matrix,
    expert_norm_scale,
    token_expert_index,
    token_expert_weight,
    expert_gate_weight,
    expert_up_weight,
    expert_down_weight,
):
    layer_out, new_state, new_hist = store(*layer(
        ep,
        hidden,
        head_input_projected,
        output_gate_projected,
        input_map_projected,
        output_map_projected,
        raw_step_size,
        jnp.swapaxes(convolution_history, 0, 1),
        convolution_kernel,
        recurrent_state_matrix,
        head_decay_rate,
        extra_log_decay,
        head_skip_weight,
        output_matrix,
        expert_norm_scale,
        token_expert_index,
        token_expert_weight,
        jnp.swapaxes(expert_gate_weight, 1, 2),
        jnp.swapaxes(expert_up_weight, 1, 2),
        expert_down_weight,
    ))
    return (layer_out, new_state, jnp.swapaxes(new_hist, 0, 1))


def solution(mesh):
    in_specs = (
        P(("grp", "ep"), "tp"),
        P(("grp", "ep"), "tp"),
        P(("grp", "ep"), "tp"),
        P(("grp", "ep"), "tp"),
        P(("grp", "ep"), "tp"),
        P(("grp", "ep"), "tp"),
        P(("grp", "ep"), None, "tp"),
        P(None, "tp"),
        P(("grp", "ep"), "tp", None, None),
        P("tp"),
        P(("grp", "ep"), "tp"),
        P("tp"),
        P("tp", None),
        P(),
        P(("grp", "ep"), None),
        P(("grp", "ep"), None),
        P("ep", None, "tp"),
        P("ep", None, "tp"),
        P("ep", "tp", None),
    )
    out_specs = (
        P(("grp", "ep"), "tp"),
        P(("grp", "ep"), "tp", None, None),
        P(("grp", "ep"), None, "tp"),
    )
    return jax.shard_map(
        functools.partial(on_device, mesh.shape["ep"]),
        mesh=mesh,
        in_specs=in_specs,
        out_specs=out_specs,
        check_vma=False,
    )
```

```python
import functools

import jax
import jax.numpy as jnp
from jax import lax
from jax.experimental import pallas as pl
from jax.experimental.pallas import tpu as pltpu
from jax.sharding import PartitionSpec as P

MESH = pl.DeviceIdType.MESH
F32 = jnp.float32
BF16 = jnp.bfloat16

STATE_DIM = 64
TOPK = 6
CAP = 2
EPSILON = 1e-06
X_SIDE = 4
FIRST = (5, -5, 2, -2, 1, -1)
RELAYS = (5, 11)
FAN = {5: (3, 2, -2, 1, -1), 11: (-2, 2, -1, 1)}
ORDER = (2, 1, 3)
LANES = 128
HIGH = lax.Precision.HIGHEST
VMEM_BYTES = 28 * 1024 * 1024


def iota(shape, dim):
    return lax.broadcasted_iota(jnp.int32, shape, dim)


def silu(v):
    return v / (1.0 + jnp.exp(-v))


def softplus(v):
    return jnp.maximum(v, 0.0) + jnp.log1p(jnp.exp(-jnp.abs(v)))


def layer_kernel(
    hidden_h, head_in_h, gate_h, b_map_h, c_map_h, raw_step_h, hist_h, taps_h, state_h, rate_h, extra_h, skip_h, wout_h,
    norm_h, chosen_h, weights_h, wg_h, wu_h, wd_h,
    out, new_state, new_hist,
    hidden, head_in, gate, b_map, c_map, raw_step, hist, taps, state, rate, extra_decay, skip, wout,
    norm, chosen, weights, wg, wu, wd,
    tp_tx, tp_rx, tokens, pick_tx, pick_rx, pick_other, down_tx, down_rx, back_tx, back_rx,
    sums, sums_bf, relay_rx, relay_tx, last_rx,
    in_sem, w_sem, tp_s, tp_r, z_s, z_r, x_s, x_r, o_s, o_r, d_s, d_r, b_s, b_r, h_s, h_r,
):
    seqs, half = hidden.shape
    nz = tokens.shape[0]
    some = nz // 2
    slots = some * CAP
    rows = X_SIDE * slots
    me, core = lax.axis_index("ep"), lax.axis_index("tp")
    z, x = me // X_SIDE, me % X_SIDE
    other = 1 - core

    def along_z(d):
        return {"ep": ((z + d + nz) % nz) * X_SIDE + x}

    def along_x(d):
        return {"ep": z * X_SIDE + (x + d) % X_SIDE}

    partner = {"tp": other}
    mine_cols = pl.ds(pl.multiple_of(core * half, half), half)
    other_cols = pl.ds(pl.multiple_of(other * half, half), half)

    barrier = pltpu.get_barrier_semaphore()
    steps = sorted({s * h for hops in (FIRST, *FAN.values()) for h in hops for s in (1, -1)})
    peers = [along_z(h) for h in steps] + [along_x(d) for d in range(1, X_SIDE)] + [partner]
    for peer in peers:
        pl.semaphore_signal(barrier, inc=1, device_id=peer, device_id_type=MESH)
    pairs = [(head_in_h, head_in), (hist_h, hist), (taps_h, taps), (raw_step_h, raw_step), (extra_h, extra_decay), (rate_h, rate),
             (skip_h, skip), (b_map_h, b_map), (c_map_h, c_map), (gate_h, gate), (hidden_h, hidden), (chosen_h, chosen),
             (weights_h, weights), (norm_h, norm)]
    small = [pltpu.make_async_copy(src, dst, in_sem.at[i]) for i, (src, dst) in enumerate(pairs)]
    for copy in small:
        copy.start()
    fetch = [pltpu.make_async_copy(state_h.at[s], state.at[s], in_sem.at[len(pairs) + s]) for s in range(seqs)]
    for copy in fetch:
        copy.start()
    get_wout = pltpu.make_async_copy(wout_h, wout, w_sem.at[0])
    get_wout.start()
    loads = [pltpu.make_async_copy(src, dst, w_sem.at[1 + i])
             for i, (src, dst) in enumerate([(wg_h.at[0], wg), (wu_h.at[0], wu), (wd_h.at[0], wd)])]
    for copy in small:
        copy.wait()

    heads = raw_step.shape[1]
    width = half // heads
    groups = b_map.shape[1] // STATE_DIM
    per_group = heads // groups
    chans = per_group * width
    fresh_in = head_in[...]
    for i in range(2):
        new_hist[i] = hist[i + 1]
    new_hist[2] = fresh_in
    kern = taps[...].astype(F32)
    total = fresh_in.astype(F32) * kern[3:4]
    for i in range(3):
        total = total + hist[i].astype(F32) * kern[i : i + 1]
    conv = silu(total)
    dt = softplus(raw_step[...].astype(F32))
    col = iota((seqs, heads), 1)
    rates = jnp.zeros((seqs, heads), F32)
    for h in range(heads):
        rates = jnp.where(col == h, rate[h], rates)
    decay = jnp.exp(-rates * dt + extra_decay[...])
    lanes_of = (iota((heads, half), 1) // width == iota((heads, half), 0)).astype(F32)
    spread = jnp.dot(jnp.concatenate([dt, decay], axis=0), lanes_of, precision=HIGH, preferred_element_type=F32)
    u = conv * spread[:seqs]
    decays = spread[seqs:]
    col = iota((seqs, half), 1) // width
    skips = jnp.zeros((seqs, half), F32)
    for h in range(heads):
        skips = jnp.where(col == h, skip[h], skips)
    opened = silu(gate[...].astype(F32))
    b_all = b_map[...].astype(F32)
    c_all = c_map[...].astype(F32)

    row_c = iota((seqs, STATE_DIM), 0)
    read = []
    for g in range(groups):
        cols = slice(g * STATE_DIM, (g + 1) * STATE_DIM)
        read.append(u[:, g * chans : (g + 1) * chans] * jnp.sum(b_all[:, cols] * c_all[:, cols], axis=1, keepdims=True))
    seen = [jnp.zeros((seqs, chans), F32) for _ in range(groups)]
    for s in range(seqs):
        fetch[s].wait()
        for g in range(groups):
            c_g = jnp.where(row_c == s, c_all[:, g * STATE_DIM : (g + 1) * STATE_DIM], 0.0).astype(BF16)
            held = state[s, g * per_group : (g + 1) * per_group].reshape(chans, STATE_DIM).astype(BF16)
            seen[g] = seen[g] + lax.dot_general(c_g, held, (((1,), (1,)), ((), ())), preferred_element_type=F32)
    for load in loads:
        load.start()
    readout = decays * jnp.concatenate(seen, axis=1) + jnp.concatenate(read, axis=1) + skips * conv
    gated = (readout * opened).astype(BF16)

    def remote(src, dst, send, recv, peer):
        return pltpu.make_async_remote_copy(
            src_ref=src, dst_ref=dst, send_sem=send, recv_sem=recv, device_id=peer, device_id_type=MESH
        )

    get_wout.wait()
    tp_tx[...] = jnp.dot(gated, wout[:, other_cols], preferred_element_type=F32).astype(BF16)
    pl.semaphore_wait(barrier, len(peers))
    swap = remote(tp_tx, tp_rx, tp_s, tp_r, partner)
    swap.start()
    own_mix = jnp.dot(gated, wout[:, mine_cols], preferred_element_type=F32).astype(BF16)

    idx = chosen[...]
    wts = weights[...]
    lane = iota((seqs, LANES), 1)
    named = jnp.zeros((seqs, LANES), F32)
    for i in range(TOPK):
        named = named + (lane == idx[:, i : i + 1]).astype(F32)
    before = (iota((seqs, seqs), 1) < iota((seqs, seqs), 0)).astype(BF16)
    rank = jnp.dot(before, named.astype(BF16), preferred_element_type=F32)
    extra = jnp.zeros((seqs, LANES), F32)
    for i in range(TOPK):
        expert = idx[:, i : i + 1]
        place = jnp.sum(jnp.where(lane == expert, rank, 0.0), axis=1, keepdims=True)
        slot = expert.astype(F32) * CAP + place
        w = wts[:, i : i + 1]
        w_hi = w.astype(BF16).astype(F32)
        extra = jnp.where(lane == i, slot, extra)
        extra = jnp.where(lane == TOPK + i, w_hi, extra)
        extra = jnp.where(lane == 2 * TOPK + i, w - w_hi, extra)
    tokens[z, :, half:] = extra.astype(BF16)

    base = hidden[...].astype(F32)
    swap.wait()
    mixed = own_mix.astype(F32) + tp_rx[...].astype(F32)
    resid = (base + mixed).astype(BF16)
    tokens[z, :, :half] = resid

    def update_states():
        u_hi = u.astype(BF16).astype(F32)
        u_t = jnp.concatenate([u_hi, u - u_hi], axis=0).T.astype(BF16)
        row = iota((2 * seqs, STATE_DIM), 0)
        for s in range(seqs):
            for g in range(groups):
                b_g = b_all[:, g * STATE_DIM : (g + 1) * STATE_DIM]
                b_g = jnp.where(row % seqs == s, jnp.concatenate([b_g, b_g], axis=0), 0.0).astype(BF16)
                outer = jnp.dot(u_t[g * chans : (g + 1) * chans], b_g, preferred_element_type=F32)
                for j in range(per_group):
                    h = g * per_group + j
                    new_state[s, h] = decay[s : s + 1, h : h + 1] * state[s, h] + outer[j * width : (j + 1) * width]

    def origin_of(back):
        return (z + nz - back) % nz

    def token_copy(back, hop):
        block = tokens.at[origin_of(back)]
        lands = (back + hop) % nz
        return remote(block, block, z_s.at[lands], z_r.at[lands], along_z(hop))

    def token_arrives(back):
        block = tokens.at[origin_of(back)]
        remote(block, block, z_s.at[back], z_r.at[back], partner).wait_recv()

    def relay(back):
        token_arrives(back)
        for hop in FAN[back]:
            token_copy(back, hop).start()

    def earlier_first(step):
        up_first = origin_of(RELAYS[0]) < origin_of(RELAYS[1])

        @pl.when(up_first)
        def _():
            step(RELAYS[0])
            step(RELAYS[1])

        @pl.when(jnp.logical_not(up_first))
        def _():
            step(RELAYS[1])
            step(RELAYS[0])

    for hop in FIRST:
        token_copy(0, hop).start()
    update_states()
    earlier_first(relay)

    def at_x(ref, part, d):
        return ref.at[part, (x + d + X_SIDE) % X_SIDE]

    def across(part):
        for origin in range(part * some, (part + 1) * some):
            back = (z + nz - origin) % nz
            awaited = back != 0
            for done in RELAYS:
                awaited = awaited & (back != done)

            @pl.when(awaited)
            def _(back=back):
                token_arrives(back)

        held = tokens[part * some : (part + 1) * some].astype(F32).reshape(some * seqs, half + LANES)
        info = held[:, half:]
        info = info + jnp.where(iota(info.shape, 1) < TOPK, 0.0, pltpu.roll(info, LANES - TOPK, 1))
        shape = (some * seqs, X_SIDE * slots)
        col = iota(shape, 1)
        slot_of = ((z * X_SIDE + col // slots) * CAP + col % CAP).astype(F32)
        same_z = (col % slots) // CAP == iota(shape, 0) // seqs
        takes = jnp.zeros(shape, F32)
        mixing = jnp.zeros(shape, F32)
        for i in range(TOPK):
            hit = same_z & (info[:, i : i + 1] == slot_of)
            takes = jnp.where(hit, 1.0, takes)
            mixing = jnp.where(hit, info[:, TOPK + i : TOPK + i + 1], mixing)
        mix_hi = mixing.astype(BF16)
        mix_lo = (mixing - mix_hi.astype(F32)).astype(BF16)
        picked = jnp.dot(takes.T.astype(BF16), held[:, :half].astype(BF16), preferred_element_type=F32).astype(BF16)
        pick_tx[part] = picked.reshape(X_SIDE, slots, half)
        sent = []
        for i, d in enumerate(ORDER):
            sent.append(remote(at_x(pick_tx, part, d), pick_rx.at[part, x], x_s.at[part, i], x_r.at[part, i], along_x(d)))
            sent[i].start()
        pick_rx[part, x] = pick_tx[part, x]
        shared = [remote(pick_tx.at[part, x], pick_other.at[part, x], o_s.at[part, 3], o_r.at[part, 3], partner)]
        shared[0].start()
        return sent, shared, (mix_hi, mix_lo)

    def share(part, shared):
        for i in (1, 2, 0):
            d = ORDER[i]
            got = at_x(pick_rx, part, -d)
            remote(got, got, x_s.at[part, i], x_r.at[part, i], along_x(d)).wait_recv()
            shared.append(remote(got, at_x(pick_other, part, -d), o_s.at[part, i], o_r.at[part, i], partner))
            shared[-1].start()

    def project(values, cols):
        f = values.reshape(rows, half).astype(F32)
        scaled = (f * norm[cols].astype(F32)[None, :]).astype(BF16)
        dims = (((1,), (1,)), ((), ()))
        g = lax.dot_general(scaled, wg[:, cols], dims, preferred_element_type=F32)
        u = lax.dot_general(scaled, wu[:, cols], dims, preferred_element_type=F32)
        return g, u, jnp.sum(f * f, axis=1, keepdims=True)

    def activate(part, shared):
        g0, u0, s0 = project(pick_rx[part], mine_cols)
        for copy in shared:
            copy.wait_recv()
        g1, u1, s1 = project(pick_other[part], other_cols)
        inv = lax.rsqrt((s0 + s1) / (2 * half) + EPSILON)
        return (silu(inv * (g0 + g1)) * (inv * (u0 + u1))).astype(BF16)

    def down(part, act):
        down_tx[part] = jnp.dot(act, wd[:, other_cols], preferred_element_type=F32).astype(BF16)
        trade = remote(down_tx.at[part], down_rx.at[part], d_s.at[part], d_r.at[part], partner)
        trade.start()
        return trade, jnp.dot(act, wd[:, mine_cols], preferred_element_type=F32).astype(BF16)

    def give_back(part, trade, own_down):
        trade.wait_recv()
        result = (own_down.astype(F32) + down_rx[part].astype(F32)).astype(BF16)
        back_tx[part] = result.reshape(X_SIDE, slots, half)
        returned = []
        for i, d in enumerate(ORDER):
            returned.append(remote(at_x(back_tx, part, d), back_rx.at[part, x], b_s.at[part, i], b_r.at[part, i], along_x(d)))
            returned[i].start()
        back_rx[part, x] = back_tx[part, x]
        return returned

    def collect(part, mix):
        for i, d in enumerate(ORDER):
            got = at_x(back_rx, part, -d)
            remote(got, got, b_s.at[part, i], b_r.at[part, i], along_x(d)).wait_recv()
        rows_back = back_rx[part].reshape(rows, half)
        total = jnp.dot(mix[0], rows_back, preferred_element_type=F32) + jnp.dot(mix[1], rows_back, preferred_element_type=F32)
        total = total.reshape(some, seqs, half)
        sums[part * some : (part + 1) * some] = total
        sums_bf[part * some : (part + 1) * some] = total.astype(BF16)

    near = [hop for hop in FIRST if hop % nz not in RELAYS]
    routes = {}
    for i, hop in enumerate(near):
        routes[hop % nz] = (-hop, last_rx.at[i])
    for back in RELAYS:
        for hop in FAN[back]:
            routes[(back + hop) % nz] = (-hop, relay_rx.at[len(routes) - len(near)])
    leaves = {back: [routes[(back + hop) % nz][1] for hop in FAN[back]] for back in RELAYS}

    def sum_copy(back):
        hop, lands = routes[back]
        return remote(sums_bf.at[origin_of(back)], lands, h_s.at[back], h_r.at[back], along_z(hop))

    def send_sums(part):
        for back in routes:

            @pl.when(origin_of(back) // some == part)
            def _(back=back):
                sum_copy(back).start()

    def relay_copy(back):
        i = RELAYS.index(back)
        hop = FIRST[i]
        return remote(relay_tx.at[i], last_rx.at[len(near) + i], h_s.at[back], h_r.at[back], along_z(-hop))

    def relay_sum(back):
        total = sums[origin_of(back)]
        for hop, landed in zip(FAN[back], leaves[back]):
            sum_copy((back + hop) % nz).wait_recv()
            total = total + landed[...].astype(F32)
        relay_tx[RELAYS.index(back)] = total.astype(BF16)
        relay_copy(back).start()

    sent_e, shared_e, mix_e = across(0)
    sent_l, shared_l, mix_l = across(1)
    share(0, shared_e)
    for load in loads:
        load.wait()
    act_e = activate(0, shared_e)
    trade_e, own_e = down(0, act_e)
    share(1, shared_l)
    act_l = activate(1, shared_l)
    trade_l, own_l = down(1, act_l)
    returned_e = give_back(0, trade_e, own_e)
    returned_l = give_back(1, trade_l, own_l)
    collect(0, mix_e)
    send_sums(0)
    collect(1, mix_l)
    send_sums(1)
    earlier_first(relay_sum)
    total = resid.astype(F32) + sums[z]
    for i, hop in enumerate(near):
        sum_copy(hop % nz).wait_recv()
        total = total + last_rx[i].astype(F32)
    for i, back in enumerate(RELAYS):
        relay_copy(back).wait_recv()
        total = total + last_rx[len(near) + i].astype(F32)
    out[...] = total.astype(BF16)

    for copy in [*sent_e, *sent_l, *shared_e, *shared_l, trade_e, trade_l, *returned_e, *returned_l]:
        copy.wait_send()
    for hop in FIRST:
        token_copy(0, hop).wait_send()
    for back in RELAYS:
        for hop in FAN[back]:
            token_copy(back, hop).wait_send()
        relay_copy(back).wait_send()
    for back in routes:
        sum_copy(back).wait_send()


def layer(ep, *args):
    hidden, head_in, gate, b_map, c_map, raw_step, hist, taps, state, rate, extra, skip, wout, norm, chosen, weights, wg, wu, wd = args
    seqs, half = hidden.shape
    nz = ep // X_SIDE
    slots = nz // 2 * CAP
    rows = X_SIDE * slots
    far = sum(len(hops) for hops in FAN.values())
    near = len(FIRST)
    vmem = pl.BlockSpec(memory_space=pltpu.VMEM)
    hbm = pl.BlockSpec(memory_space=pltpu.HBM)
    dma = pltpu.SemaphoreType.DMA
    one = dma(())

    def room(a):
        return pltpu.VMEM(a.shape, a.dtype)

    return pl.pallas_call(
        layer_kernel,
        name="layer",
        in_specs=[hbm] * len(args),
        out_specs=[vmem, vmem, vmem],
        out_shape=[
            pltpu.VMEM(hidden.shape, BF16),
            pltpu.VMEM(state.shape, F32),
            pltpu.VMEM(hist.shape, BF16),
        ],
        scratch_shapes=[
            *(pltpu.SMEM(a.shape, F32) if a is rate or a is skip else room(a) for a in args[:16]),
            *(pltpu.VMEM(a.shape[1:], BF16) for a in (wg, wu, wd)),
            room(hidden),
            room(hidden),
            pltpu.VMEM((nz, seqs, half + LANES), BF16),
            *(pltpu.VMEM((2, X_SIDE, slots, half), BF16) for _ in range(3)),
            *(pltpu.VMEM((2, rows, half), BF16) for _ in range(2)),
            *(pltpu.VMEM((2, X_SIDE, slots, half), BF16) for _ in range(2)),
            pltpu.VMEM((nz, seqs, half), F32),
            pltpu.VMEM((nz, seqs, half), BF16),
            pltpu.VMEM((far, seqs, half), BF16),
            pltpu.VMEM((2, seqs, half), BF16),
            pltpu.VMEM((near, seqs, half), BF16),
            dma((14 + seqs,)), dma((4,)), one, one, dma((nz,)), dma((nz,)), dma((2, 3)), dma((2, 3)), dma((2, 4)), dma((2, 4)),
            dma((2,)), dma((2,)), dma((2, 3)), dma((2, 3)), dma((nz,)), dma((nz,)),
        ],
        compiler_params=pltpu.CompilerParams(collective_id=0, has_side_effects=True, vmem_limit_bytes=VMEM_BYTES),
    )(*(pltpu.with_memory_space_constraint(a, pltpu.HBM) for a in args))


def store_kernel(*refs):
    count = (len(refs) - 1) // 2
    sem = refs[-1]
    copies = [pltpu.make_async_copy(refs[i], refs[count + i], sem.at[i]) for i in range(count)]
    for copy in copies:
        copy.start()
    for copy in copies:
        copy.wait()


def store(*values):
    return pl.pallas_call(
        store_kernel,
        name="store",
        in_specs=[pl.BlockSpec(memory_space=pltpu.VMEM)] * len(values),
        out_specs=[pl.BlockSpec(memory_space=pltpu.HBM)] * len(values),
        out_shape=[pltpu.HBM(v.shape, v.dtype) for v in values],
        scratch_shapes=[pltpu.SemaphoreType.DMA((len(values),))],
        compiler_params=pltpu.CompilerParams(vmem_limit_bytes=VMEM_BYTES),
    )(*(pltpu.with_memory_space_constraint(v, pltpu.VMEM) for v in values))


def on_device(
    ep,
    hidden,
    head_input_projected,
    output_gate_projected,
    input_map_projected,
    output_map_projected,
    raw_step_size,
    convolution_history,
    convolution_kernel,
    recurrent_state_matrix,
    head_decay_rate,
    extra_log_decay,
    head_skip_weight,
    output_matrix,
    expert_norm_scale,
    token_expert_index,
    token_expert_weight,
    expert_gate_weight,
    expert_up_weight,
    expert_down_weight,
):
    layer_out, new_state, new_hist = store(*layer(
        ep,
        hidden,
        head_input_projected,
        output_gate_projected,
        input_map_projected,
        output_map_projected,
        raw_step_size,
        jnp.swapaxes(convolution_history, 0, 1),
        convolution_kernel,
        recurrent_state_matrix,
        head_decay_rate,
        extra_log_decay,
        head_skip_weight,
        output_matrix,
        expert_norm_scale,
        token_expert_index,
        token_expert_weight,
        jnp.swapaxes(expert_gate_weight, 1, 2),
        jnp.swapaxes(expert_up_weight, 1, 2),
        expert_down_weight,
    ))
    return (layer_out, new_state, jnp.swapaxes(new_hist, 0, 1))


def solution(mesh):
    in_specs = (
        P(("grp", "ep"), "tp"),
        P(("grp", "ep"), "tp"),
        P(("grp", "ep"), "tp"),
        P(("grp", "ep"), "tp"),
        P(("grp", "ep"), "tp"),
        P(("grp", "ep"), "tp"),
        P(("grp", "ep"), None, "tp"),
        P(None, "tp"),
        P(("grp", "ep"), "tp", None, None),
        P("tp"),
        P(("grp", "ep"), "tp"),
        P("tp"),
        P("tp", None),
        P(),
        P(("grp", "ep"), None),
        P(("grp", "ep"), None),
        P("ep", None, "tp"),
        P("ep", None, "tp"),
        P("ep", "tp", None),
    )
    out_specs = (
        P(("grp", "ep"), "tp"),
        P(("grp", "ep"), "tp", None, None),
        P(("grp", "ep"), None, "tp"),
    )
    return jax.shard_map(
        functools.partial(on_device, mesh.shape["ep"]),
        mesh=mesh,
        in_specs=in_specs,
        out_specs=out_specs,
        check_vma=False,
    )
```

```python
import functools

import jax
import jax.numpy as jnp
from jax import lax
from jax.experimental import pallas as pl
from jax.experimental.pallas import tpu as pltpu
from jax.sharding import PartitionSpec as P

MESH = pl.DeviceIdType.MESH
F32 = jnp.float32
BF16 = jnp.bfloat16

STATE_DIM = 64
TOPK = 6
CAP = 2
EPSILON = 1e-06
X_SIDE = 4
FIRST = [(0, (4, -4, 3, -3, 2, -2, 1, -1))]
FAN = [(4, (4, 3, 2, 1)), (12, (-3, -2, -1))]
BLOCKS = (0, 1, 15, 2, 14, 4, 12, 3, 13, 5, 6, 7, 8, 9, 10, 11)
PLACE = {block: place for place, block in enumerate(BLOCKS)}
ORDER = (2, 1, 3)
LANES = 128
HIGH = lax.Precision.HIGHEST
VMEM_BYTES = 28 * 1024 * 1024


def iota(shape, dim):
    return lax.broadcasted_iota(jnp.int32, shape, dim)


def silu(v):
    return v / (1.0 + jnp.exp(-v))


def softplus(v):
    return jnp.maximum(v, 0.0) + jnp.log1p(jnp.exp(-jnp.abs(v)))


def layer_kernel(
    hidden_h, head_in_h, gate_h, b_map_h, c_map_h, raw_step_h, hist_h, taps_h, state_h, rate_h, extra_h, skip_h, wout_h,
    norm_h, chosen_h, weights_h, wg_h, wu_h, wd_h,
    out_h, new_state_h, new_hist_h,
    out, new_state, new_hist, hidden, head_in, gate, b_map, c_map, raw_step, hist, taps, state, rate, extra_decay, skip, wout,
    norm, chosen, weights, wg, wu, wd,
    tp_tx, tp_rx, tokens, pick_tx, pick_rx, pick_other, down_tx, down_rx, back_tx, back_rx,
    sums, sums_bf, relay_rx, relay_tx, last_rx,
    in_sem, w_sem, tp_s, tp_r, z_s, z_r, x_s, x_r, o_s, o_r, d_s, d_r, b_s, b_r, h_s, h_r,
):
    seqs, half = hidden.shape
    nz = tokens.shape[0]
    some = nz // 2
    slots = some * CAP
    rows = X_SIDE * slots
    me, core = lax.axis_index("ep"), lax.axis_index("tp")
    z, x = me // X_SIDE, me % X_SIDE
    other = 1 - core

    def along_z(d):
        return {"ep": ((z + d + nz) % nz) * X_SIDE + x}

    def along_x(d):
        return {"ep": z * X_SIDE + (x + d) % X_SIDE}

    partner = {"tp": other}
    mine_cols = pl.ds(pl.multiple_of(core * half, half), half)
    other_cols = pl.ds(pl.multiple_of(other * half, half), half)

    pairs = [(c_map_h, c_map), (head_in_h, head_in), (hist_h, hist), (taps_h, taps), (raw_step_h, raw_step), (extra_h, extra_decay),
             (rate_h, rate), (skip_h, skip), (b_map_h, b_map), (gate_h, gate), (hidden_h, hidden), (chosen_h, chosen),
             (weights_h, weights), (norm_h, norm)]
    small = [pltpu.make_async_copy(src, dst, in_sem.at[i]) for i, (src, dst) in enumerate(pairs)]
    two = seqs // 4
    fetch = [pltpu.make_async_copy(state_h.at[pl.ds(i * two, two)], state.at[pl.ds(i * two, two)], in_sem.at[len(pairs) + i]) for i in range(4)]
    get_wout = pltpu.make_async_copy(wout_h, wout, w_sem.at[0])
    loads = [pltpu.make_async_copy(src, dst, w_sem.at[1 + i])
             for i, (src, dst) in enumerate([(wg_h.at[0], wg), (wu_h.at[0], wu), (wd_h.at[0], wd)])]
    for copy in [small[0], *fetch, *small[1:], get_wout]:
        copy.start()
    barrier = pltpu.get_barrier_semaphore()
    steps = sorted({s * h for _, hops in FIRST + FAN for h in hops for s in (1, -1)})
    peers = [along_z(h) for h in steps] + [along_x(d) for d in range(1, X_SIDE)] + [partner]
    for peer in peers:
        pl.semaphore_signal(barrier, inc=1, device_id=peer, device_id_type=MESH)

    heads = raw_step.shape[1]
    width = half // heads
    groups = b_map.shape[1] // STATE_DIM
    per_group = heads // groups
    chans = per_group * width
    small[0].wait()
    c_all = c_map[...].astype(F32)
    row_c = iota((seqs, STATE_DIM), 0)
    seen = [jnp.zeros((seqs, chans), F32) for _ in range(groups)]
    for s in range(seqs):
        if s % two == 0:
            fetch[s // two].wait()
        for g in range(groups):
            c_g = jnp.where(row_c == s, c_all[:, g * STATE_DIM : (g + 1) * STATE_DIM], 0.0).astype(BF16)
            held = state[s, g * per_group : (g + 1) * per_group].reshape(chans, STATE_DIM).astype(BF16)
            seen[g] = seen[g] + lax.dot_general(c_g, held, (((1,), (1,)), ((), ())), preferred_element_type=F32)
    for copy in small[1:]:
        copy.wait()

    fresh_in = head_in[...]
    for i in range(2):
        new_hist[i] = hist[i + 1]
    new_hist[2] = fresh_in
    kern = taps[...].astype(F32)
    total = fresh_in.astype(F32) * kern[3:4]
    for i in range(3):
        total = total + hist[i].astype(F32) * kern[i : i + 1]
    conv = silu(total)
    dt = softplus(raw_step[...].astype(F32))
    col = iota((seqs, heads), 1)
    rates = jnp.zeros((seqs, heads), F32)
    for h in range(heads):
        rates = jnp.where(col == h, rate[h], rates)
    decay = jnp.exp(-rates * dt + extra_decay[...])
    lanes_of = (iota((heads, half), 1) // width == iota((heads, half), 0)).astype(F32)
    spread = jnp.dot(jnp.concatenate([dt, decay], axis=0), lanes_of, precision=HIGH, preferred_element_type=F32)
    u = conv * spread[:seqs]
    decays = spread[seqs:]
    col = iota((seqs, half), 1) // width
    skips = jnp.zeros((seqs, half), F32)
    for h in range(heads):
        skips = jnp.where(col == h, skip[h], skips)
    opened = silu(gate[...].astype(F32))
    b_all = b_map[...].astype(F32)
    read = []
    for g in range(groups):
        cols = slice(g * STATE_DIM, (g + 1) * STATE_DIM)
        read.append(u[:, g * chans : (g + 1) * chans] * jnp.sum(b_all[:, cols] * c_all[:, cols], axis=1, keepdims=True))
    for load in loads:
        load.start()
    readout = decays * jnp.concatenate(seen, axis=1) + jnp.concatenate(read, axis=1) + skips * conv
    gated = (readout * opened).astype(BF16)

    def remote(src, dst, send, recv, peer):
        return pltpu.make_async_remote_copy(
            src_ref=src, dst_ref=dst, send_sem=send, recv_sem=recv, device_id=peer, device_id_type=MESH
        )

    get_wout.wait()
    tp_tx[...] = jnp.dot(gated, wout[:, other_cols], preferred_element_type=F32).astype(BF16)
    pl.semaphore_wait(barrier, len(peers))
    swap = remote(tp_tx, tp_rx, tp_s, tp_r, partner)
    swap.start()
    own_mix = jnp.dot(gated, wout[:, mine_cols], preferred_element_type=F32).astype(BF16)

    idx = chosen[...]
    wts = weights[...]
    lane = iota((seqs, LANES), 1)
    named = jnp.zeros((seqs, LANES), F32)
    for i in range(TOPK):
        named = named + (lane == idx[:, i : i + 1]).astype(F32)
    before = (iota((seqs, seqs), 1) < iota((seqs, seqs), 0)).astype(BF16)
    rank = jnp.dot(before, named.astype(BF16), preferred_element_type=F32)
    extra = jnp.zeros((seqs, LANES), F32)
    for i in range(TOPK):
        expert = idx[:, i : i + 1]
        place = jnp.sum(jnp.where(lane == expert, rank, 0.0), axis=1, keepdims=True)
        slot = expert.astype(F32) * CAP + place
        w = wts[:, i : i + 1]
        w_hi = w.astype(BF16).astype(F32)
        extra = jnp.where(lane == i, slot, extra)
        extra = jnp.where(lane == TOPK + i, w_hi, extra)
        extra = jnp.where(lane == 2 * TOPK + i, w - w_hi, extra)
    tokens[0, :, half:] = extra.astype(BF16)

    base = hidden[...].astype(F32)
    swap.wait()
    mixed = own_mix.astype(F32) + tp_rx[...].astype(F32)
    resid = (base + mixed).astype(BF16)
    tokens[0, :, :half] = resid

    def update_states():
        u_hi = u.astype(BF16).astype(F32)
        u_t = jnp.concatenate([u_hi, u - u_hi], axis=0).T.astype(BF16)
        row = iota((2 * seqs, STATE_DIM), 0)
        for s in range(seqs):
            for g in range(groups):
                b_g = b_all[:, g * STATE_DIM : (g + 1) * STATE_DIM]
                b_g = jnp.where(row % seqs == s, jnp.concatenate([b_g, b_g], axis=0), 0.0).astype(BF16)
                outer = jnp.dot(u_t[g * chans : (g + 1) * chans], b_g, preferred_element_type=F32)
                for j in range(per_group):
                    h = g * per_group + j
                    new_state[s, h] = decay[s : s + 1, h : h + 1] * state[s, h] + outer[j * width : (j + 1) * width]

    copies, arrived = [], {}

    def spread_from(origin, hops):
        for hop in hops:
            q = len(copies)
            lands = (origin + hop) % nz
            copies.append(remote(tokens.at[PLACE[origin]], tokens.at[PLACE[lands]], z_s.at[q], z_r.at[q], along_z(hop)))
            arrived[lands] = copies[q]
            copies[q].start()

    for origin, hops in FIRST:
        spread_from(origin, hops)
    update_states()
    keep = [pltpu.make_async_copy(new_state, new_state_h, w_sem.at[4]), pltpu.make_async_copy(new_hist, new_hist_h, w_sem.at[5]),
            pltpu.make_async_copy(out, out_h, w_sem.at[6])]
    for copy in keep[:2]:
        copy.start()
    for origin, hops in FAN:
        arrived.pop(origin).wait_recv()
        spread_from(origin, hops)

    def at_x(ref, part, d):
        return ref.at[part, (x + d + X_SIDE) % X_SIDE]

    def across(part):
        for place in range(part * some, (part + 1) * some):
            if BLOCKS[place] in arrived:
                arrived.pop(BLOCKS[place]).wait_recv()
        held = tokens[part * some : (part + 1) * some].astype(F32).reshape(some * seqs, half + LANES)
        info = held[:, half:]
        info = info + jnp.where(iota(info.shape, 1) < TOPK, 0.0, pltpu.roll(info, LANES - TOPK, 1))
        shape = (some * seqs, X_SIDE * slots)
        col = iota(shape, 1)
        slot_of = ((z * X_SIDE + col // slots) * CAP + col % CAP).astype(F32)
        same_z = (col % slots) // CAP == iota(shape, 0) // seqs
        takes = jnp.zeros(shape, F32)
        mixing = jnp.zeros(shape, F32)
        for i in range(TOPK):
            hit = same_z & (info[:, i : i + 1] == slot_of)
            takes = jnp.where(hit, 1.0, takes)
            mixing = jnp.where(hit, info[:, TOPK + i : TOPK + i + 1], mixing)
        mix_hi = mixing.astype(BF16)
        mix_lo = (mixing - mix_hi.astype(F32)).astype(BF16)
        picked = jnp.dot(takes.T.astype(BF16), held[:, :half].astype(BF16), preferred_element_type=F32).astype(BF16)
        pick_tx[part] = picked.reshape(X_SIDE, slots, half)
        sent = []
        for i, d in enumerate(ORDER):
            sent.append(remote(at_x(pick_tx, part, d), pick_rx.at[part, x], x_s.at[part, i], x_r.at[part, i], along_x(d)))
            sent[i].start()
        pick_rx[part, x] = pick_tx[part, x]
        shared = [remote(pick_tx.at[part, x], pick_other.at[part, x], o_s.at[part, 3], o_r.at[part, 3], partner)]
        shared[0].start()
        return sent, shared, (mix_hi, mix_lo)

    def share(part, shared):
        for i in (1, 2, 0):
            d = ORDER[i]
            got = at_x(pick_rx, part, -d)
            remote(got, got, x_s.at[part, i], x_r.at[part, i], along_x(d)).wait_recv()
            shared.append(remote(got, at_x(pick_other, part, -d), o_s.at[part, i], o_r.at[part, i], partner))
            shared[-1].start()

    def project(values, cols):
        f = values.reshape(rows, half).astype(F32)
        scaled = (f * norm[cols].astype(F32)[None, :]).astype(BF16)
        dims = (((1,), (1,)), ((), ()))
        g = lax.dot_general(scaled, wg[:, cols], dims, preferred_element_type=F32)
        u = lax.dot_general(scaled, wu[:, cols], dims, preferred_element_type=F32)
        return g, u, jnp.sum(f * f, axis=1, keepdims=True)

    def activate(part, shared):
        g0, u0, s0 = project(pick_rx[part], mine_cols)
        for copy in shared:
            copy.wait_recv()
        g1, u1, s1 = project(pick_other[part], other_cols)
        inv = lax.rsqrt((s0 + s1) / (2 * half) + EPSILON)
        return (silu(inv * (g0 + g1)) * (inv * (u0 + u1))).astype(BF16)

    def down(part, act):
        down_tx[part] = jnp.dot(act, wd[:, other_cols], preferred_element_type=F32).astype(BF16)
        trade = remote(down_tx.at[part], down_rx.at[part], d_s.at[part], d_r.at[part], partner)
        trade.start()
        return trade, jnp.dot(act, wd[:, mine_cols], preferred_element_type=F32).astype(BF16)

    def back(part, trade, own_down):
        trade.wait_recv()
        result = (own_down.astype(F32) + down_rx[part].astype(F32)).astype(BF16)
        back_tx[part] = result.reshape(X_SIDE, slots, half)
        returned = []
        for i, d in enumerate(ORDER):
            returned.append(remote(at_x(back_tx, part, d), back_rx.at[part, x], b_s.at[part, i], b_r.at[part, i], along_x(d)))
            returned[i].start()
        back_rx[part, x] = back_tx[part, x]
        return returned

    def collect(part, mix):
        for i, d in enumerate(ORDER):
            got = at_x(back_rx, part, -d)
            remote(got, got, b_s.at[part, i], b_r.at[part, i], along_x(d)).wait_recv()
        rows_back = back_rx[part].reshape(rows, half)
        total = jnp.dot(mix[0], rows_back, preferred_element_type=F32) + jnp.dot(mix[1], rows_back, preferred_element_type=F32)
        total = total.reshape(some, seqs, half)
        sums[part * some : (part + 1) * some] = total
        sums_bf[part * some : (part + 1) * some] = total.astype(BF16)

    sent_n, shared_n, mix_n = across(0)
    sent_f, shared_f, mix_f = across(1)
    share(0, shared_n)
    for load in loads:
        load.wait()
    act_n = activate(0, shared_n)
    share(1, shared_f)
    act_f = activate(1, shared_f)
    trade_f, own_f = down(1, act_f)
    trade_n, own_n = down(0, act_n)
    returned_f = back(1, trade_f, own_f)
    returned_n = back(0, trade_n, own_n)

    parts = []

    def send(src, dst, hop):
        q = len(parts)
        parts.append(remote(src, dst, h_s.at[q], h_r.at[q], along_z(hop)))
        parts[q].start()
        return parts[q]

    gathered = {origin: [] for origin, _ in FAN}

    def send_far(part):
        for origin, hops in FAN:
            for hop in hops:
                place = PLACE[(origin + hop) % nz]
                if place // some == part:
                    n = sum(len(g) for g in gathered.values())
                    gathered[origin].append((send(sums_bf.at[place], relay_rx.at[n], -hop), n))

    collect(1, mix_f)
    send_far(1)
    collect(0, mix_n)
    send_far(0)
    finals = []
    (_, first_hops), = FIRST
    for hop in first_hops[len(FAN):]:
        finals.append(send(sums_bf.at[PLACE[hop % nz]], last_rx.at[len(finals)], -hop))
    for i, (origin, _) in enumerate(FAN):
        total = sums[PLACE[origin]]
        for copy, at in gathered[origin]:
            copy.wait_recv()
            total = total + relay_rx[at].astype(F32)
        relay_tx[i] = total.astype(BF16)
        finals.append(send(relay_tx.at[i], last_rx.at[len(finals)], -first_hops[i]))
    total = resid.astype(F32) + sums[0]
    for i, copy in enumerate(finals):
        copy.wait_recv()
        total = total + last_rx[i].astype(F32)
    out[...] = total.astype(BF16)
    keep[2].start()
    for copy in [*copies, *sent_n, *sent_f, *shared_n, *shared_f, trade_n, trade_f, *returned_n, *returned_f, *parts]:
        copy.wait_send()
    for copy in keep:
        copy.wait()


def layer(ep, *args):
    hidden, head_in, gate, b_map, c_map, raw_step, hist, taps, state, rate, extra, skip, wout, norm, chosen, weights, wg, wu, wd = args
    seqs, half = hidden.shape
    nz = ep // X_SIDE
    slots = nz // 2 * CAP
    rows = X_SIDE * slots
    far = sum(len(hops) for _, hops in FAN)
    near = len(FIRST[0][1])
    vmem = pl.BlockSpec(memory_space=pltpu.VMEM)
    hbm = pl.BlockSpec(memory_space=pltpu.HBM)
    dma = pltpu.SemaphoreType.DMA
    one = dma(())

    def room(a):
        return pltpu.VMEM(a.shape, a.dtype)

    return pl.pallas_call(
        layer_kernel,
        name="layer",
        in_specs=[hbm] * len(args),
        out_specs=[pl.BlockSpec(memory_space=pl.ANY)] * 3,
        out_shape=[
            pltpu.VMEM(hidden.shape, BF16),
            pltpu.VMEM(state.shape, F32),
            pltpu.VMEM(hist.shape, BF16),
        ],
        scratch_shapes=[
            room(hidden),
            room(state),
            room(hist),
            *(pltpu.SMEM(a.shape, F32) if a is rate or a is skip else room(a) for a in args[:16]),
            *(pltpu.VMEM(a.shape[1:], BF16) for a in (wg, wu, wd)),
            room(hidden),
            room(hidden),
            pltpu.VMEM((nz, seqs, half + LANES), BF16),
            *(pltpu.VMEM((2, X_SIDE, slots, half), BF16) for _ in range(3)),
            *(pltpu.VMEM((2, rows, half), BF16) for _ in range(2)),
            *(pltpu.VMEM((2, X_SIDE, slots, half), BF16) for _ in range(2)),
            pltpu.VMEM((nz, seqs, half), F32),
            pltpu.VMEM((nz, seqs, half), BF16),
            pltpu.VMEM((far, seqs, half), BF16),
            pltpu.VMEM((2, seqs, half), BF16),
            pltpu.VMEM((near, seqs, half), BF16),
            dma((14 + seqs,)), dma((7,)), one, one, dma((nz - 1,)), dma((nz - 1,)), dma((2, 3)), dma((2, 3)), dma((2, 4)), dma((2, 4)),
            dma((2,)), dma((2,)), dma((2, 3)), dma((2, 3)), dma((nz - 1,)), dma((nz - 1,)),
        ],
        compiler_params=pltpu.CompilerParams(collective_id=0, has_side_effects=True, vmem_limit_bytes=VMEM_BYTES),
    )(*(pltpu.with_memory_space_constraint(a, pltpu.HBM) for a in args))


def store_kernel(*refs):
    count = (len(refs) - 1) // 2
    sem = refs[-1]
    copies = []
    for src, dst in zip(refs[:count], refs[count:-1]):
        pieces = src.shape[0] if src.ndim == 4 else 1
        for i in range(pieces):
            piece = pl.ds(i * (src.shape[0] // pieces), src.shape[0] // pieces)
            copies.append(pltpu.make_async_copy(src.at[piece], dst.at[piece], sem.at[len(copies)]))
            copies[-1].start()
    for copy in copies:
        copy.wait()


def store(*values):
    return pl.pallas_call(
        store_kernel,
        name="store",
        in_specs=[pl.BlockSpec(memory_space=pl.ANY)] * len(values),
        out_specs=[pl.BlockSpec(memory_space=pltpu.HBM)] * len(values),
        out_shape=[pltpu.HBM(v.shape, v.dtype) for v in values],
        scratch_shapes=[pltpu.SemaphoreType.DMA((sum(v.shape[0] for v in values),))],
        compiler_params=pltpu.CompilerParams(vmem_limit_bytes=VMEM_BYTES),
    )(*(pltpu.with_memory_space_constraint(v, pltpu.VMEM) for v in values))


def on_device(
    ep,
    hidden,
    head_input_projected,
    output_gate_projected,
    input_map_projected,
    output_map_projected,
    raw_step_size,
    convolution_history,
    convolution_kernel,
    recurrent_state_matrix,
    head_decay_rate,
    extra_log_decay,
    head_skip_weight,
    output_matrix,
    expert_norm_scale,
    token_expert_index,
    token_expert_weight,
    expert_gate_weight,
    expert_up_weight,
    expert_down_weight,
):
    layer_out, new_state, new_hist = store(*layer(
        ep,
        hidden,
        head_input_projected,
        output_gate_projected,
        input_map_projected,
        output_map_projected,
        raw_step_size,
        jnp.swapaxes(convolution_history, 0, 1),
        convolution_kernel,
        recurrent_state_matrix,
        head_decay_rate,
        extra_log_decay,
        head_skip_weight,
        output_matrix,
        expert_norm_scale,
        token_expert_index,
        token_expert_weight,
        jnp.swapaxes(expert_gate_weight, 1, 2),
        jnp.swapaxes(expert_up_weight, 1, 2),
        expert_down_weight,
    ))
    return (layer_out, new_state, jnp.swapaxes(new_hist, 0, 1))


def solution(mesh):
    in_specs = (
        P(("grp", "ep"), "tp"),
        P(("grp", "ep"), "tp"),
        P(("grp", "ep"), "tp"),
        P(("grp", "ep"), "tp"),
        P(("grp", "ep"), "tp"),
        P(("grp", "ep"), "tp"),
        P(("grp", "ep"), None, "tp"),
        P(None, "tp"),
        P(("grp", "ep"), "tp", None, None),
        P("tp"),
        P(("grp", "ep"), "tp"),
        P("tp"),
        P("tp", None),
        P(),
        P(("grp", "ep"), None),
        P(("grp", "ep"), None),
        P("ep", None, "tp"),
        P("ep", None, "tp"),
        P("ep", "tp", None),
    )
    out_specs = (
        P(("grp", "ep"), "tp"),
        P(("grp", "ep"), "tp", None, None),
        P(("grp", "ep"), None, "tp"),
    )
    return jax.shard_map(
        functools.partial(on_device, mesh.shape["ep"]),
        mesh=mesh,
        in_specs=in_specs,
        out_specs=out_specs,
        check_vma=False,
    )
```

```python
import functools

import jax
import jax.numpy as jnp
from jax import lax
from jax.experimental import pallas as pl
from jax.experimental.pallas import tpu as pltpu
from jax.sharding import PartitionSpec as P

MESH = pl.DeviceIdType.MESH
F32 = jnp.float32
BF16 = jnp.bfloat16

STATE_DIM = 64
TOPK = 6
CAP = 2
EPSILON = 1e-06
X_SIDE = 4
FIRST = [(0, (4, -4, 3, -3, 2, -2, 1, -1))]
FAN = [(4, (4, 3, 2, 1)), (12, (-3, -2, -1))]
BLOCKS = (0, 1, 15, 2, 14, 4, 12, 3, 13, 5, 6, 7, 8, 9, 10, 11)
PLACE = {block: place for place, block in enumerate(BLOCKS)}
ORDER = (2, 1, 3)
LANES = 128
HIGH = lax.Precision.HIGHEST
VMEM_BYTES = 28 * 1024 * 1024


def iota(shape, dim):
    return lax.broadcasted_iota(jnp.int32, shape, dim)


def silu(v):
    return v / (1.0 + jnp.exp(-v))


def softplus(v):
    return jnp.maximum(v, 0.0) + jnp.log1p(jnp.exp(-jnp.abs(v)))


def layer_kernel(
    hidden_h, head_in_h, gate_h, b_map_h, c_map_h, raw_step_h, hist_h, taps_h, state_h, rate_h, extra_h, skip_h, wout_h,
    norm_h, chosen_h, weights_h, wg_h, wu_h, wd_h,
    out_h, new_state_h, new_hist_h,
    out, new_state, new_hist, hidden, head_in, gate, b_map, c_map, raw_step, hist, taps, state, rate, extra_decay, skip, wout,
    norm, chosen, weights, wg, wu, wd,
    tp_tx, tp_rx, tokens, pick_tx, pick_rx, pick_other, down_tx, down_rx, back_tx, back_rx,
    sums, sums_bf, relay_rx, relay_tx, last_rx,
    in_sem, w_sem, tp_s, tp_r, z_s, z_r, x_s, x_r, o_s, o_r, d_s, d_r, b_s, b_r, h_s, h_r,
):
    seqs, half = hidden.shape
    nz = tokens.shape[0]
    some = nz // 2
    slots = some * CAP
    rows = X_SIDE * slots
    me, core = lax.axis_index("ep"), lax.axis_index("tp")
    z, x = me // X_SIDE, me % X_SIDE
    other = 1 - core
    turn = 1 - 2 * core

    def spot(block):
        here, there = PLACE[block], PLACE[(nz - block) % nz]
        return here if here == there else jnp.where(core == 0, here, there)

    def along_z(d):
        return {"ep": ((z + turn * d + nz) % nz) * X_SIDE + x}

    def along_x(d):
        return {"ep": z * X_SIDE + (x + d) % X_SIDE}

    partner = {"tp": other}
    mine_cols = pl.ds(pl.multiple_of(core * half, half), half)
    other_cols = pl.ds(pl.multiple_of(other * half, half), half)

    pairs = [(c_map_h, c_map), (head_in_h, head_in), (hist_h, hist), (taps_h, taps), (raw_step_h, raw_step), (extra_h, extra_decay),
             (rate_h, rate), (skip_h, skip), (b_map_h, b_map), (gate_h, gate), (hidden_h, hidden), (chosen_h, chosen),
             (weights_h, weights), (norm_h, norm)]
    small = [pltpu.make_async_copy(src, dst, in_sem.at[i]) for i, (src, dst) in enumerate(pairs)]
    two = seqs // 4
    fetch = [pltpu.make_async_copy(state_h.at[pl.ds(i * two, two)], state.at[pl.ds(i * two, two)], in_sem.at[len(pairs) + i]) for i in range(4)]
    get_wout = pltpu.make_async_copy(wout_h, wout, w_sem.at[0])
    loads = [pltpu.make_async_copy(src, dst, w_sem.at[1 + i])
             for i, (src, dst) in enumerate([(wg_h.at[0], wg), (wu_h.at[0], wu), (wd_h.at[0], wd)])]
    for copy in [small[0], *fetch, *small[1:], get_wout]:
        copy.start()
    barrier = pltpu.get_barrier_semaphore()
    steps = sorted({s * h for _, hops in FIRST + FAN for h in hops for s in (1, -1)})
    peers = [along_z(h) for h in steps] + [along_x(d) for d in range(1, X_SIDE)] + [partner]
    for peer in peers:
        pl.semaphore_signal(barrier, inc=1, device_id=peer, device_id_type=MESH)

    heads = raw_step.shape[1]
    width = half // heads
    groups = b_map.shape[1] // STATE_DIM
    per_group = heads // groups
    chans = per_group * width
    small[0].wait()
    c_all = c_map[...].astype(F32)
    row_c = iota((seqs, STATE_DIM), 0)
    seen = [jnp.zeros((seqs, chans), F32) for _ in range(groups)]
    for s in range(seqs):
        if s % two == 0:
            fetch[s // two].wait()
        for g in range(groups):
            c_g = jnp.where(row_c == s, c_all[:, g * STATE_DIM : (g + 1) * STATE_DIM], 0.0).astype(BF16)
            held = state[s, g * per_group : (g + 1) * per_group].reshape(chans, STATE_DIM).astype(BF16)
            seen[g] = seen[g] + lax.dot_general(c_g, held, (((1,), (1,)), ((), ())), preferred_element_type=F32)
    for copy in small[1:]:
        copy.wait()

    fresh_in = head_in[...]
    for i in range(2):
        new_hist[i] = hist[i + 1]
    new_hist[2] = fresh_in
    kern = taps[...].astype(F32)
    total = fresh_in.astype(F32) * kern[3:4]
    for i in range(3):
        total = total + hist[i].astype(F32) * kern[i : i + 1]
    conv = silu(total)
    dt = softplus(raw_step[...].astype(F32))
    col = iota((seqs, heads), 1)
    rates = jnp.zeros((seqs, heads), F32)
    for h in range(heads):
        rates = jnp.where(col == h, rate[h], rates)
    decay = jnp.exp(-rates * dt + extra_decay[...])
    lanes_of = (iota((heads, half), 1) // width == iota((heads, half), 0)).astype(F32)
    spread = jnp.dot(jnp.concatenate([dt, decay], axis=0), lanes_of, precision=HIGH, preferred_element_type=F32)
    u = conv * spread[:seqs]
    decays = spread[seqs:]
    col = iota((seqs, half), 1) // width
    skips = jnp.zeros((seqs, half), F32)
    for h in range(heads):
        skips = jnp.where(col == h, skip[h], skips)
    opened = silu(gate[...].astype(F32))
    b_all = b_map[...].astype(F32)
    read = []
    for g in range(groups):
        cols = slice(g * STATE_DIM, (g + 1) * STATE_DIM)
        read.append(u[:, g * chans : (g + 1) * chans] * jnp.sum(b_all[:, cols] * c_all[:, cols], axis=1, keepdims=True))
    for load in loads:
        load.start()
    readout = decays * jnp.concatenate(seen, axis=1) + jnp.concatenate(read, axis=1) + skips * conv
    gated = (readout * opened).astype(BF16)

    def remote(src, dst, send, recv, peer):
        return pltpu.make_async_remote_copy(
            src_ref=src, dst_ref=dst, send_sem=send, recv_sem=recv, device_id=peer, device_id_type=MESH
        )

    get_wout.wait()
    tp_tx[...] = jnp.dot(gated, wout[:, other_cols], preferred_element_type=F32).astype(BF16)
    pl.semaphore_wait(barrier, len(peers))
    swap = remote(tp_tx, tp_rx, tp_s, tp_r, partner)
    swap.start()
    own_mix = jnp.dot(gated, wout[:, mine_cols], preferred_element_type=F32).astype(BF16)

    idx = chosen[...]
    wts = weights[...]
    lane = iota((seqs, LANES), 1)
    named = jnp.zeros((seqs, LANES), F32)
    for i in range(TOPK):
        named = named + (lane == idx[:, i : i + 1]).astype(F32)
    before = (iota((seqs, seqs), 1) < iota((seqs, seqs), 0)).astype(BF16)
    rank = jnp.dot(before, named.astype(BF16), preferred_element_type=F32)
    extra = jnp.zeros((seqs, LANES), F32)
    for i in range(TOPK):
        expert = idx[:, i : i + 1]
        place = jnp.sum(jnp.where(lane == expert, rank, 0.0), axis=1, keepdims=True)
        slot = expert.astype(F32) * CAP + place
        w = wts[:, i : i + 1]
        w_hi = w.astype(BF16).astype(F32)
        extra = jnp.where(lane == i, slot, extra)
        extra = jnp.where(lane == TOPK + i, w_hi, extra)
        extra = jnp.where(lane == 2 * TOPK + i, w - w_hi, extra)
    tokens[0, :, half:] = extra.astype(BF16)

    base = hidden[...].astype(F32)
    swap.wait()
    mixed = own_mix.astype(F32) + tp_rx[...].astype(F32)
    resid = (base + mixed).astype(BF16)
    tokens[0, :, :half] = resid

    def update_states():
        u_hi = u.astype(BF16).astype(F32)
        u_t = jnp.concatenate([u_hi, u - u_hi], axis=0).T.astype(BF16)
        row = iota((2 * seqs, STATE_DIM), 0)
        for s in range(seqs):
            for g in range(groups):
                b_g = b_all[:, g * STATE_DIM : (g + 1) * STATE_DIM]
                b_g = jnp.where(row % seqs == s, jnp.concatenate([b_g, b_g], axis=0), 0.0).astype(BF16)
                outer = jnp.dot(u_t[g * chans : (g + 1) * chans], b_g, preferred_element_type=F32)
                for j in range(per_group):
                    h = g * per_group + j
                    new_state[s, h] = decay[s : s + 1, h : h + 1] * state[s, h] + outer[j * width : (j + 1) * width]

    copies, arrived = [], {}

    def spread_from(origin, hops):
        for hop in hops:
            q = len(copies)
            lands = (origin + hop) % nz
            copies.append(remote(tokens.at[spot(origin)], tokens.at[spot(lands)], z_s.at[q], z_r.at[q], along_z(hop)))
            arrived[lands] = copies[q]
            copies[q].start()

    for origin, hops in FIRST:
        spread_from(origin, hops)
    update_states()
    keep = [pltpu.make_async_copy(new_state, new_state_h, w_sem.at[4]), pltpu.make_async_copy(new_hist, new_hist_h, w_sem.at[5]),
            pltpu.make_async_copy(out, out_h, w_sem.at[6])]
    for copy in keep[:2]:
        copy.start()
    for origin, hops in FAN:
        arrived.pop(origin).wait_recv()
        spread_from(origin, hops)

    def at_x(ref, part, d):
        return ref.at[part, (x + d + X_SIDE) % X_SIDE]

    def across(part):
        for block in [b for b in arrived if part or {b, nz - b} & set(BLOCKS[:some])]:
            arrived.pop(block).wait_recv()
        held = tokens[part * some : (part + 1) * some].astype(F32).reshape(some * seqs, half + LANES)
        info = held[:, half:]
        info = info + jnp.where(iota(info.shape, 1) < TOPK, 0.0, pltpu.roll(info, LANES - TOPK, 1))
        shape = (some * seqs, X_SIDE * slots)
        col = iota(shape, 1)
        slot_of = ((z * X_SIDE + col // slots) * CAP + col % CAP).astype(F32)
        same_z = (col % slots) // CAP == iota(shape, 0) // seqs
        takes = jnp.zeros(shape, F32)
        mixing = jnp.zeros(shape, F32)
        for i in range(TOPK):
            hit = same_z & (info[:, i : i + 1] == slot_of)
            takes = jnp.where(hit, 1.0, takes)
            mixing = jnp.where(hit, info[:, TOPK + i : TOPK + i + 1], mixing)
        mix_hi = mixing.astype(BF16)
        mix_lo = (mixing - mix_hi.astype(F32)).astype(BF16)
        picked = jnp.dot(takes.T.astype(BF16), held[:, :half].astype(BF16), preferred_element_type=F32).astype(BF16)
        pick_tx[part] = picked.reshape(X_SIDE, slots, half)
        sent = []
        for i, d in enumerate(ORDER):
            sent.append(remote(at_x(pick_tx, part, d), pick_rx.at[part, x], x_s.at[part, i], x_r.at[part, i], along_x(d)))
            sent[i].start()
        pick_rx[part, x] = pick_tx[part, x]
        shared = [remote(pick_tx.at[part, x], pick_other.at[part, x], o_s.at[part, 3], o_r.at[part, 3], partner)]
        shared[0].start()
        return sent, shared, (mix_hi, mix_lo)

    def share(part, shared):
        for i in (1, 2, 0):
            d = ORDER[i]
            got = at_x(pick_rx, part, -d)
            remote(got, got, x_s.at[part, i], x_r.at[part, i], along_x(d)).wait_recv()
            shared.append(remote(got, at_x(pick_other, part, -d), o_s.at[part, i], o_r.at[part, i], partner))
            shared[-1].start()

    def project(values, cols):
        f = values.reshape(rows, half).astype(F32)
        scaled = (f * norm[cols].astype(F32)[None, :]).astype(BF16)
        dims = (((1,), (1,)), ((), ()))
        g = lax.dot_general(scaled, wg[:, cols], dims, preferred_element_type=F32)
        u = lax.dot_general(scaled, wu[:, cols], dims, preferred_element_type=F32)
        return g, u, jnp.sum(f * f, axis=1, keepdims=True)

    def activate(part, shared):
        g0, u0, s0 = project(pick_rx[part], mine_cols)
        for copy in shared:
            copy.wait_recv()
        g1, u1, s1 = project(pick_other[part], other_cols)
        inv = lax.rsqrt((s0 + s1) / (2 * half) + EPSILON)
        return (silu(inv * (g0 + g1)) * (inv * (u0 + u1))).astype(BF16)

    def down(part, act):
        down_tx[part] = jnp.dot(act, wd[:, other_cols], preferred_element_type=F32).astype(BF16)
        trade = remote(down_tx.at[part], down_rx.at[part], d_s.at[part], d_r.at[part], partner)
        trade.start()
        return trade, jnp.dot(act, wd[:, mine_cols], preferred_element_type=F32).astype(BF16)

    def back(part, trade, own_down):
        trade.wait_recv()
        result = (own_down.astype(F32) + down_rx[part].astype(F32)).astype(BF16)
        back_tx[part] = result.reshape(X_SIDE, slots, half)
        returned = []
        for i, d in enumerate(ORDER):
            returned.append(remote(at_x(back_tx, part, d), back_rx.at[part, x], b_s.at[part, i], b_r.at[part, i], along_x(d)))
            returned[i].start()
        back_rx[part, x] = back_tx[part, x]
        return returned

    def collect(part, mix):
        for i, d in enumerate(ORDER):
            got = at_x(back_rx, part, -d)
            remote(got, got, b_s.at[part, i], b_r.at[part, i], along_x(d)).wait_recv()
        rows_back = back_rx[part].reshape(rows, half)
        total = jnp.dot(mix[0], rows_back, preferred_element_type=F32) + jnp.dot(mix[1], rows_back, preferred_element_type=F32)
        total = total.reshape(some, seqs, half)
        sums[part * some : (part + 1) * some] = total
        sums_bf[part * some : (part + 1) * some] = total.astype(BF16)

    sent_n, shared_n, mix_n = across(0)
    sent_f, shared_f, mix_f = across(1)
    share(0, shared_n)
    for load in loads:
        load.wait()
    act_n = activate(0, shared_n)
    share(1, shared_f)
    act_f = activate(1, shared_f)
    trade_f, own_f = down(1, act_f)
    trade_n, own_n = down(0, act_n)
    returned_f = back(1, trade_f, own_f)
    returned_n = back(0, trade_n, own_n)

    parts = []

    def send(src, dst, hop):
        q = len(parts)
        parts.append(remote(src, dst, h_s.at[q], h_r.at[q], along_z(hop)))
        parts[q].start()
        return parts[q]

    gathered = {origin: [] for origin, _ in FAN}

    def send_far(part):
        for origin, hops in FAN:
            for hop in hops:
                block = (origin + hop) % nz
                if PLACE[block] // some == part:
                    n = sum(len(g) for g in gathered.values())
                    gathered[origin].append((send(sums_bf.at[spot(block)], relay_rx.at[n], -hop), n))

    collect(1, mix_f)
    send_far(1)
    collect(0, mix_n)
    send_far(0)
    finals = []
    (_, first_hops), = FIRST
    for i, (origin, _) in enumerate(FAN):
        total = sums[spot(origin)]
        for copy, at in gathered[origin]:
            copy.wait_recv()
            total = total + relay_rx[at].astype(F32)
        relay_tx[i] = total.astype(BF16)
        finals.append(send(relay_tx.at[i], last_rx.at[len(finals)], -first_hops[i]))
    for hop in first_hops[len(FAN):]:
        finals.append(send(sums_bf.at[spot(hop % nz)], last_rx.at[len(finals)], -hop))
    total = resid.astype(F32) + sums[0]
    for i, copy in enumerate(finals):
        copy.wait_recv()
        total = total + last_rx[i].astype(F32)
    out[...] = total.astype(BF16)
    keep[2].start()
    for copy in [*copies, *sent_n, *sent_f, *shared_n, *shared_f, trade_n, trade_f, *returned_n, *returned_f, *parts]:
        copy.wait_send()
    for copy in keep:
        copy.wait()


def layer(ep, *args):
    hidden, head_in, gate, b_map, c_map, raw_step, hist, taps, state, rate, extra, skip, wout, norm, chosen, weights, wg, wu, wd = args
    seqs, half = hidden.shape
    nz = ep // X_SIDE
    slots = nz // 2 * CAP
    rows = X_SIDE * slots
    far = sum(len(hops) for _, hops in FAN)
    near = len(FIRST[0][1])
    vmem = pl.BlockSpec(memory_space=pltpu.VMEM)
    hbm = pl.BlockSpec(memory_space=pltpu.HBM)
    dma = pltpu.SemaphoreType.DMA
    one = dma(())

    def room(a):
        return pltpu.VMEM(a.shape, a.dtype)

    return pl.pallas_call(
        layer_kernel,
        name="layer",
        in_specs=[hbm] * len(args),
        out_specs=[pl.BlockSpec(memory_space=pl.ANY)] * 3,
        out_shape=[
            pltpu.VMEM(hidden.shape, BF16),
            pltpu.VMEM(state.shape, F32),
            pltpu.VMEM(hist.shape, BF16),
        ],
        scratch_shapes=[
            room(hidden),
            room(state),
            room(hist),
            *(pltpu.SMEM(a.shape, F32) if a is rate or a is skip else room(a) for a in args[:16]),
            *(pltpu.VMEM(a.shape[1:], BF16) for a in (wg, wu, wd)),
            room(hidden),
            room(hidden),
            pltpu.VMEM((nz, seqs, half + LANES), BF16),
            *(pltpu.VMEM((2, X_SIDE, slots, half), BF16) for _ in range(3)),
            *(pltpu.VMEM((2, rows, half), BF16) for _ in range(2)),
            *(pltpu.VMEM((2, X_SIDE, slots, half), BF16) for _ in range(2)),
            pltpu.VMEM((nz, seqs, half), F32),
            pltpu.VMEM((nz, seqs, half), BF16),
            pltpu.VMEM((far, seqs, half), BF16),
            pltpu.VMEM((2, seqs, half), BF16),
            pltpu.VMEM((near, seqs, half), BF16),
            dma((14 + seqs,)), dma((7,)), one, one, dma((nz - 1,)), dma((nz - 1,)), dma((2, 3)), dma((2, 3)), dma((2, 4)), dma((2, 4)),
            dma((2,)), dma((2,)), dma((2, 3)), dma((2, 3)), dma((nz - 1,)), dma((nz - 1,)),
        ],
        compiler_params=pltpu.CompilerParams(collective_id=0, has_side_effects=True, vmem_limit_bytes=VMEM_BYTES),
    )(*(pltpu.with_memory_space_constraint(a, pltpu.HBM) for a in args))


def store_kernel(*refs):
    count = (len(refs) - 1) // 2
    sem = refs[-1]
    copies = []
    for src, dst in zip(refs[:count], refs[count:-1]):
        pieces = src.shape[0] if src.ndim == 4 else 1
        for i in range(pieces):
            piece = pl.ds(i * (src.shape[0] // pieces), src.shape[0] // pieces)
            copies.append(pltpu.make_async_copy(src.at[piece], dst.at[piece], sem.at[len(copies)]))
            copies[-1].start()
    for copy in copies:
        copy.wait()


def store(*values):
    return pl.pallas_call(
        store_kernel,
        name="store",
        in_specs=[pl.BlockSpec(memory_space=pl.ANY)] * len(values),
        out_specs=[pl.BlockSpec(memory_space=pltpu.HBM)] * len(values),
        out_shape=[pltpu.HBM(v.shape, v.dtype) for v in values],
        scratch_shapes=[pltpu.SemaphoreType.DMA((sum(v.shape[0] for v in values),))],
        compiler_params=pltpu.CompilerParams(vmem_limit_bytes=VMEM_BYTES),
    )(*(pltpu.with_memory_space_constraint(v, pltpu.VMEM) for v in values))


def on_device(
    ep,
    hidden,
    head_input_projected,
    output_gate_projected,
    input_map_projected,
    output_map_projected,
    raw_step_size,
    convolution_history,
    convolution_kernel,
    recurrent_state_matrix,
    head_decay_rate,
    extra_log_decay,
    head_skip_weight,
    output_matrix,
    expert_norm_scale,
    token_expert_index,
    token_expert_weight,
    expert_gate_weight,
    expert_up_weight,
    expert_down_weight,
):
    layer_out, new_state, new_hist = store(*layer(
        ep,
        hidden,
        head_input_projected,
        output_gate_projected,
        input_map_projected,
        output_map_projected,
        raw_step_size,
        jnp.swapaxes(convolution_history, 0, 1),
        convolution_kernel,
        recurrent_state_matrix,
        head_decay_rate,
        extra_log_decay,
        head_skip_weight,
        output_matrix,
        expert_norm_scale,
        token_expert_index,
        token_expert_weight,
        jnp.swapaxes(expert_gate_weight, 1, 2),
        jnp.swapaxes(expert_up_weight, 1, 2),
        expert_down_weight,
    ))
    return (layer_out, new_state, jnp.swapaxes(new_hist, 0, 1))


def solution(mesh):
    in_specs = (
        P(("grp", "ep"), "tp"),
        P(("grp", "ep"), "tp"),
        P(("grp", "ep"), "tp"),
        P(("grp", "ep"), "tp"),
        P(("grp", "ep"), "tp"),
        P(("grp", "ep"), "tp"),
        P(("grp", "ep"), None, "tp"),
        P(None, "tp"),
        P(("grp", "ep"), "tp", None, None),
        P("tp"),
        P(("grp", "ep"), "tp"),
        P("tp"),
        P("tp", None),
        P(),
        P(("grp", "ep"), None),
        P(("grp", "ep"), None),
        P("ep", None, "tp"),
        P("ep", None, "tp"),
        P("ep", "tp", None),
    )
    out_specs = (
        P(("grp", "ep"), "tp"),
        P(("grp", "ep"), "tp", None, None),
        P(("grp", "ep"), None, "tp"),
    )
    return jax.shard_map(
        functools.partial(on_device, mesh.shape["ep"]),
        mesh=mesh,
        in_specs=in_specs,
        out_specs=out_specs,
        check_vma=False,
    )
```

```python
import functools

import jax
import jax.numpy as jnp
from jax import lax
from jax.experimental import pallas as pl
from jax.experimental.pallas import tpu as pltpu
from jax.sharding import PartitionSpec as P

MESH = pl.DeviceIdType.MESH
F32 = jnp.float32
BF16 = jnp.bfloat16

STATE_DIM = 64
TOPK = 6
CAP = 2
EPSILON = 1e-06
X_SIDE = 4
FIRST = [(0, (4, -4, 3, -3, 2, -2, 1, -1))]
FAN = [(4, (4, 3, 2, 1)), (12, (-3, -2, -1))]
BLOCKS = (0, 1, 15, 2, 14, 4, 12, 3, 13, 5, 6, 7, 8, 9, 10, 11)
PLACE = {block: place for place, block in enumerate(BLOCKS)}
ORDER = (2, 1, 3)
LANES = 128
HIGH = lax.Precision.HIGHEST
VMEM_BYTES = 28 * 1024 * 1024


def iota(shape, dim):
    return lax.broadcasted_iota(jnp.int32, shape, dim)


def silu(v):
    return v / (1.0 + jnp.exp(-v))


def softplus(v):
    return jnp.maximum(v, 0.0) + jnp.log1p(jnp.exp(-jnp.abs(v)))


def layer_kernel(
    hidden_h, head_in_h, gate_h, b_map_h, c_map_h, raw_step_h, hist_h, taps_h, state_h, rate_h, extra_h, skip_h, wout_h,
    norm_h, chosen_h, weights_h, wg_h, wu_h, wd_h,
    out_h, new_state_h, new_hist_h,
    out, new_state, new_hist, hidden, head_in, gate, b_map, c_map, raw_step, hist, taps, state, rate, extra_decay, skip, wout,
    norm, chosen, weights, wg, wu, wd,
    tp_tx, tp_rx, tokens, pick_tx, pick_rx, pick_other, down_tx, down_rx, back_tx, back_rx,
    sums, sums_bf, relay_rx, relay_tx, last_rx,
    in_sem, w_sem, tp_s, tp_r, z_s, z_r, x_s, x_r, o_s, o_r, d_s, d_r, b_s, b_r, h_s, h_r,
):
    seqs, half = hidden.shape
    nz = tokens.shape[0]
    some = nz // 2
    slots = some * CAP
    rows = X_SIDE * slots
    me, core = lax.axis_index("ep"), lax.axis_index("tp")
    z, x = me // X_SIDE, me % X_SIDE
    other = 1 - core
    turn = 1 - 2 * core

    def spot(block):
        here, there = PLACE[block], PLACE[(nz - block) % nz]
        return here if here == there else jnp.where(core == 0, here, there)

    def along_z(d):
        return {"ep": ((z + turn * d + nz) % nz) * X_SIDE + x}

    def along_x(d):
        return {"ep": z * X_SIDE + (x + d) % X_SIDE}

    partner = {"tp": other}
    mine_cols = pl.ds(pl.multiple_of(core * half, half), half)
    other_cols = pl.ds(pl.multiple_of(other * half, half), half)

    pairs = [(c_map_h, c_map), (head_in_h, head_in), (hist_h, hist), (taps_h, taps), (raw_step_h, raw_step), (extra_h, extra_decay),
             (rate_h, rate), (skip_h, skip), (b_map_h, b_map), (gate_h, gate), (hidden_h, hidden), (chosen_h, chosen),
             (weights_h, weights), (norm_h, norm)]
    small = [pltpu.make_async_copy(src, dst, in_sem.at[i]) for i, (src, dst) in enumerate(pairs)]
    two = seqs // 4
    fetch = [pltpu.make_async_copy(state_h.at[pl.ds(i * two, two)], state.at[pl.ds(i * two, two)], in_sem.at[len(pairs) + i]) for i in range(4)]
    get_wout = pltpu.make_async_copy(wout_h, wout, w_sem.at[0])
    loads = [pltpu.make_async_copy(src, dst, w_sem.at[1 + i])
             for i, (src, dst) in enumerate([(wg_h.at[0], wg), (wu_h.at[0], wu), (wd_h.at[0], wd)])]
    for copy in [small[0], *fetch, *small[1:], get_wout]:
        copy.start()
    barrier = pltpu.get_barrier_semaphore()
    steps = sorted({s * h for _, hops in FIRST + FAN for h in hops for s in (1, -1)})
    peers = [along_z(h) for h in steps] + [along_x(d) for d in range(1, X_SIDE)] + [partner]
    for peer in peers:
        pl.semaphore_signal(barrier, inc=1, device_id=peer, device_id_type=MESH)

    heads = raw_step.shape[1]
    width = half // heads
    groups = b_map.shape[1] // STATE_DIM
    per_group = heads // groups
    chans = per_group * width
    small[0].wait()
    c_all = c_map[...].astype(F32)
    row_c = iota((seqs, STATE_DIM), 0)
    seen = [jnp.zeros((seqs, chans), F32) for _ in range(groups)]
    for s in range(seqs):
        if s % two == 0:
            fetch[s // two].wait()
        for g in range(groups):
            c_g = jnp.where(row_c == s, c_all[:, g * STATE_DIM : (g + 1) * STATE_DIM], 0.0).astype(BF16)
            held = state[s, g * per_group : (g + 1) * per_group].reshape(chans, STATE_DIM).astype(BF16)
            seen[g] = seen[g] + lax.dot_general(c_g, held, (((1,), (1,)), ((), ())), preferred_element_type=F32)
    for copy in small[1:]:
        copy.wait()

    fresh_in = head_in[...]
    for i in range(2):
        new_hist[i] = hist[i + 1]
    new_hist[2] = fresh_in
    kern = taps[...].astype(F32)
    total = fresh_in.astype(F32) * kern[3:4]
    for i in range(3):
        total = total + hist[i].astype(F32) * kern[i : i + 1]
    conv = silu(total)
    dt = softplus(raw_step[...].astype(F32))
    col = iota((seqs, heads), 1)
    rates = jnp.zeros((seqs, heads), F32)
    for h in range(heads):
        rates = jnp.where(col == h, rate[h], rates)
    decay = jnp.exp(-rates * dt + extra_decay[...])
    lanes_of = (iota((heads, half), 1) // width == iota((heads, half), 0)).astype(F32)
    spread = jnp.dot(jnp.concatenate([dt, decay], axis=0), lanes_of, precision=HIGH, preferred_element_type=F32)
    u = conv * spread[:seqs]
    decays = spread[seqs:]
    col = iota((seqs, half), 1) // width
    skips = jnp.zeros((seqs, half), F32)
    for h in range(heads):
        skips = jnp.where(col == h, skip[h], skips)
    opened = silu(gate[...].astype(F32))
    b_all = b_map[...].astype(F32)
    read = []
    for g in range(groups):
        cols = slice(g * STATE_DIM, (g + 1) * STATE_DIM)
        read.append(u[:, g * chans : (g + 1) * chans] * jnp.sum(b_all[:, cols] * c_all[:, cols], axis=1, keepdims=True))
    for load in loads:
        load.start()
    readout = decays * jnp.concatenate(seen, axis=1) + jnp.concatenate(read, axis=1) + skips * conv
    gated = (readout * opened).astype(BF16)

    def remote(src, dst, send, recv, peer):
        return pltpu.make_async_remote_copy(
            src_ref=src, dst_ref=dst, send_sem=send, recv_sem=recv, device_id=peer, device_id_type=MESH
        )

    get_wout.wait()
    tp_tx[...] = jnp.dot(gated, wout[:, other_cols], preferred_element_type=F32).astype(BF16)
    pl.semaphore_wait(barrier, len(peers))
    swap = remote(tp_tx, tp_rx, tp_s, tp_r, partner)
    swap.start()
    own_mix = jnp.dot(gated, wout[:, mine_cols], preferred_element_type=F32).astype(BF16)

    idx = chosen[...]
    wts = weights[...]
    lane = iota((seqs, LANES), 1)
    named = jnp.zeros((seqs, LANES), F32)
    for i in range(TOPK):
        named = named + (lane == idx[:, i : i + 1]).astype(F32)
    before = (iota((seqs, seqs), 1) < iota((seqs, seqs), 0)).astype(BF16)
    rank = jnp.dot(before, named.astype(BF16), preferred_element_type=F32)
    extra = jnp.zeros((seqs, LANES), F32)
    for i in range(TOPK):
        expert = idx[:, i : i + 1]
        place = jnp.sum(jnp.where(lane == expert, rank, 0.0), axis=1, keepdims=True)
        slot = expert.astype(F32) * CAP + place
        w = wts[:, i : i + 1]
        w_hi = w.astype(BF16).astype(F32)
        extra = jnp.where(lane == i, slot, extra)
        extra = jnp.where(lane == TOPK + i, w_hi, extra)
        extra = jnp.where(lane == 2 * TOPK + i, w - w_hi, extra)
    tokens[0, :, half:] = extra.astype(BF16)

    base = hidden[...].astype(F32)
    swap.wait()
    mixed = own_mix.astype(F32) + tp_rx[...].astype(F32)
    resid = (base + mixed).astype(BF16)
    tokens[0, :, :half] = resid

    def update_states():
        u_hi = u.astype(BF16).astype(F32)
        u_t = jnp.concatenate([u_hi, u - u_hi], axis=0).T.astype(BF16)
        row = iota((2 * seqs, STATE_DIM), 0)
        for s in range(seqs):
            for g in range(groups):
                b_g = b_all[:, g * STATE_DIM : (g + 1) * STATE_DIM]
                b_g = jnp.where(row % seqs == s, jnp.concatenate([b_g, b_g], axis=0), 0.0).astype(BF16)
                outer = jnp.dot(u_t[g * chans : (g + 1) * chans], b_g, preferred_element_type=F32)
                for j in range(per_group):
                    h = g * per_group + j
                    new_state[s, h] = decay[s : s + 1, h : h + 1] * state[s, h] + outer[j * width : (j + 1) * width]

    direct = [hop % nz for hop in FIRST[0][1] if hop % nz not in [origin for origin, _ in FAN]]

    def first_for(block):
        for i, (origin, _) in enumerate(FAN):
            if block == origin:
                return i
        return 2 if block in direct else 3

    def token_wait(count, at):
        some_blocks = tokens.at[pl.ds(0, count)]
        return remote(some_blocks, some_blocks, z_s, z_r.at[at], partner)

    def spread_from(origin, hops):
        for hop in hops:
            lands = (origin + hop) % nz
            remote(tokens.at[spot(origin)], tokens.at[spot(lands)], z_s, z_r.at[first_for(lands)], along_z(hop)).start()

    for origin, hops in FIRST:
        spread_from(origin, hops)
    update_states()
    keep = [pltpu.make_async_copy(new_state, new_state_h, w_sem.at[4]), pltpu.make_async_copy(new_hist, new_hist_h, w_sem.at[5]),
            pltpu.make_async_copy(out, out_h, w_sem.at[6])]
    for copy in keep[:2]:
        copy.start()
    for origin, hops in FAN:
        token_wait(1, first_for(origin)).wait_recv()
        spread_from(origin, hops)

    def at_x(ref, part, d):
        return ref.at[part, (x + d + X_SIDE) % X_SIDE]

    def across(part):
        if part:
            token_wait(nz - 1 - len(FAN) - len(direct), 3).wait_recv()
        else:
            token_wait(len(direct), 2).wait_recv()
        held = tokens[part * some : (part + 1) * some].astype(F32).reshape(some * seqs, half + LANES)
        info = held[:, half:]
        info = info + jnp.where(iota(info.shape, 1) < TOPK, 0.0, pltpu.roll(info, LANES - TOPK, 1))
        shape = (some * seqs, X_SIDE * slots)
        col = iota(shape, 1)
        slot_of = ((z * X_SIDE + col // slots) * CAP + col % CAP).astype(F32)
        same_z = (col % slots) // CAP == iota(shape, 0) // seqs
        takes = jnp.zeros(shape, F32)
        mixing = jnp.zeros(shape, F32)
        for i in range(TOPK):
            hit = same_z & (info[:, i : i + 1] == slot_of)
            takes = jnp.where(hit, 1.0, takes)
            mixing = jnp.where(hit, info[:, TOPK + i : TOPK + i + 1], mixing)
        mix_hi = mixing.astype(BF16)
        mix_lo = (mixing - mix_hi.astype(F32)).astype(BF16)
        picked = jnp.dot(takes.T.astype(BF16), held[:, :half].astype(BF16), preferred_element_type=F32).astype(BF16)
        pick_tx[part] = picked.reshape(X_SIDE, slots, half)
        sent = []
        for i, d in enumerate(ORDER):
            sent.append(remote(at_x(pick_tx, part, d), pick_rx.at[part, x], x_s.at[part], x_r.at[part, i], along_x(d)))
            sent[i].start()
        pick_rx[part, x] = pick_tx[part, x]
        shared = [remote(pick_tx.at[part, x], pick_other.at[part, x], o_s.at[part], o_r.at[part], partner)]
        shared[0].start()
        return sent, shared, (mix_hi, mix_lo)

    def share(part, shared):
        for i in (1, 2, 0):
            d = ORDER[i]
            got = at_x(pick_rx, part, -d)
            remote(got, got, x_s.at[part], x_r.at[part, i], along_x(d)).wait_recv()
            shared.append(remote(got, at_x(pick_other, part, -d), o_s.at[part], o_r.at[part], partner))
            shared[-1].start()

    def project(values, cols):
        f = values.reshape(rows, half).astype(F32)
        scaled = (f * norm[cols].astype(F32)[None, :]).astype(BF16)
        dims = (((1,), (1,)), ((), ()))
        g = lax.dot_general(scaled, wg[:, cols], dims, preferred_element_type=F32)
        u = lax.dot_general(scaled, wu[:, cols], dims, preferred_element_type=F32)
        return g, u, jnp.sum(f * f, axis=1, keepdims=True)

    def activate(part, shared):
        g0, u0, s0 = project(pick_rx[part], mine_cols)
        remote(pick_rx.at[part], pick_other.at[part], o_s.at[part], o_r.at[part], partner).wait_recv()
        g1, u1, s1 = project(pick_other[part], other_cols)
        inv = lax.rsqrt((s0 + s1) / (2 * half) + EPSILON)
        return (silu(inv * (g0 + g1)) * (inv * (u0 + u1))).astype(BF16)

    def down(part, act):
        down_tx[part] = jnp.dot(act, wd[:, other_cols], preferred_element_type=F32).astype(BF16)
        trade = remote(down_tx.at[part], down_rx.at[part], d_s.at[part], d_r.at[part], partner)
        trade.start()
        return trade, jnp.dot(act, wd[:, mine_cols], preferred_element_type=F32).astype(BF16)

    def back(part, trade, own_down):
        trade.wait_recv()
        result = (own_down.astype(F32) + down_rx[part].astype(F32)).astype(BF16)
        back_tx[part] = result.reshape(X_SIDE, slots, half)
        returned = []
        for i, d in enumerate(ORDER):
            returned.append(remote(at_x(back_tx, part, d), back_rx.at[part, x], b_s.at[part], b_r.at[part], along_x(d)))
            returned[i].start()
        back_rx[part, x] = back_tx[part, x]
        return returned

    def three_backs(part):
        blocks = pl.ds(0, X_SIDE - 1)
        return remote(back_tx.at[part, blocks], back_rx.at[part, blocks], b_s.at[part], b_r.at[part], partner)

    def collect(part, mix):
        three_backs(part).wait_recv()
        rows_back = back_rx[part].reshape(rows, half)
        total = jnp.dot(mix[0], rows_back, preferred_element_type=F32) + jnp.dot(mix[1], rows_back, preferred_element_type=F32)
        total = total.reshape(some, seqs, half)
        sums[part * some : (part + 1) * some] = total
        sums_bf[part * some : (part + 1) * some] = total.astype(BF16)

    sent_n, shared_n, mix_n = across(0)
    sent_f, shared_f, mix_f = across(1)
    share(0, shared_n)
    for load in loads:
        load.wait()
    act_n = activate(0, shared_n)
    share(1, shared_f)
    act_f = activate(1, shared_f)
    trade_f, own_f = down(1, act_f)
    trade_n, own_n = down(0, act_n)
    returned_f = back(1, trade_f, own_f)
    returned_n = back(0, trade_n, own_n)

    def send(src, dst, hop, at):
        remote(src, dst, h_s, h_r.at[at], along_z(hop)).start()

    def sum_wait(count, at):
        some_blocks = sums_bf.at[pl.ds(0, count)]
        return remote(some_blocks, some_blocks, h_s, h_r.at[at], partner)

    (_, first_hops), = FIRST
    counts = [len(hops) for _, hops in FAN]

    collect(1, mix_f)
    for i, (origin, hops) in enumerate(FAN):
        for n, hop in enumerate(hops):
            send(sums_bf.at[spot((origin + hop) % nz)], relay_rx.at[sum(counts[:i]) + n], -hop, i)
    collect(0, mix_n)
    for i, (origin, hops) in enumerate(FAN):
        sum_wait(counts[i], i).wait_recv()
        total = sums[spot(origin)]
        for n in range(counts[i]):
            total = total + relay_rx[sum(counts[:i]) + n].astype(F32)
        relay_tx[i] = total.astype(BF16)
        send(relay_tx.at[i], last_rx.at[i], -first_hops[i], 2)
    for i, hop in enumerate(first_hops[len(FAN) :]):
        send(sums_bf.at[spot(hop % nz)], last_rx.at[len(FAN) + i], -hop, 2)
    total = resid.astype(F32) + sums[0]
    sum_wait(len(first_hops), 2).wait_recv()
    for i in range(len(first_hops)):
        total = total + last_rx[i].astype(F32)
    out[...] = total.astype(BF16)
    keep[2].start()
    token_wait(nz - 1, 0).wait_send()
    sum_wait(nz - 1, 0).wait_send()
    for part in range(2):
        three = pick_tx.at[part, pl.ds(0, X_SIDE - 1)]
        remote(three, three, x_s.at[part], x_r.at[part, 0], partner).wait_send()
        remote(pick_rx.at[part], pick_other.at[part], o_s.at[part], o_r.at[part], partner).wait_send()
        three_backs(part).wait_send()
    trade_n.wait_send()
    trade_f.wait_send()
    for copy in keep:
        copy.wait()


def layer(ep, *args):
    hidden, head_in, gate, b_map, c_map, raw_step, hist, taps, state, rate, extra, skip, wout, norm, chosen, weights, wg, wu, wd = args
    seqs, half = hidden.shape
    nz = ep // X_SIDE
    slots = nz // 2 * CAP
    rows = X_SIDE * slots
    far = sum(len(hops) for _, hops in FAN)
    near = len(FIRST[0][1])
    vmem = pl.BlockSpec(memory_space=pltpu.VMEM)
    hbm = pl.BlockSpec(memory_space=pltpu.HBM)
    dma = pltpu.SemaphoreType.DMA
    one = dma(())

    def room(a):
        return pltpu.VMEM(a.shape, a.dtype)

    return pl.pallas_call(
        layer_kernel,
        name="layer",
        in_specs=[hbm] * len(args),
        out_specs=[pl.BlockSpec(memory_space=pl.ANY)] * 3,
        out_shape=[
            pltpu.VMEM(hidden.shape, BF16),
            pltpu.VMEM(state.shape, F32),
            pltpu.VMEM(hist.shape, BF16),
        ],
        scratch_shapes=[
            room(hidden),
            room(state),
            room(hist),
            *(pltpu.SMEM(a.shape, F32) if a is rate or a is skip else room(a) for a in args[:16]),
            *(pltpu.VMEM(a.shape[1:], BF16) for a in (wg, wu, wd)),
            room(hidden),
            room(hidden),
            pltpu.VMEM((nz, seqs, half + LANES), BF16),
            *(pltpu.VMEM((2, X_SIDE, slots, half), BF16) for _ in range(3)),
            *(pltpu.VMEM((2, rows, half), BF16) for _ in range(2)),
            *(pltpu.VMEM((2, X_SIDE, slots, half), BF16) for _ in range(2)),
            pltpu.VMEM((nz, seqs, half), F32),
            pltpu.VMEM((nz, seqs, half), BF16),
            pltpu.VMEM((far, seqs, half), BF16),
            pltpu.VMEM((2, seqs, half), BF16),
            pltpu.VMEM((near, seqs, half), BF16),
            dma((14 + 4,)), dma((7,)), one, one, one, dma((4,)), dma((2,)), dma((2, 3)), dma((2,)), dma((2,)),
            dma((2,)), dma((2,)), dma((2,)), dma((2,)), one, dma((3,)),
        ],
        compiler_params=pltpu.CompilerParams(collective_id=0, has_side_effects=True, vmem_limit_bytes=VMEM_BYTES),
    )(*(pltpu.with_memory_space_constraint(a, pltpu.HBM) for a in args))


def store_kernel(*refs):
    count = (len(refs) - 1) // 2
    pairs = list(zip(refs[:count], refs[count:-1]))
    for at, (src, dst) in enumerate(pairs):
        pieces = src.shape[0] if src.ndim == 4 else 1
        for i in range(pieces):
            piece = pl.ds(i * (src.shape[0] // pieces), src.shape[0] // pieces)
            pltpu.make_async_copy(src.at[piece], dst.at[piece], refs[-1].at[at]).start()
    for at, (src, dst) in enumerate(pairs):
        pltpu.make_async_copy(src, dst, refs[-1].at[at]).wait()


def store(*values):
    return pl.pallas_call(
        store_kernel,
        name="store",
        in_specs=[pl.BlockSpec(memory_space=pl.ANY)] * len(values),
        out_specs=[pl.BlockSpec(memory_space=pltpu.HBM)] * len(values),
        out_shape=[pltpu.HBM(v.shape, v.dtype) for v in values],
        scratch_shapes=[pltpu.SemaphoreType.DMA((len(values),))],
        compiler_params=pltpu.CompilerParams(vmem_limit_bytes=VMEM_BYTES),
    )(*(pltpu.with_memory_space_constraint(v, pltpu.VMEM) for v in values))


def on_device(
    ep,
    hidden,
    head_input_projected,
    output_gate_projected,
    input_map_projected,
    output_map_projected,
    raw_step_size,
    convolution_history,
    convolution_kernel,
    recurrent_state_matrix,
    head_decay_rate,
    extra_log_decay,
    head_skip_weight,
    output_matrix,
    expert_norm_scale,
    token_expert_index,
    token_expert_weight,
    expert_gate_weight,
    expert_up_weight,
    expert_down_weight,
):
    layer_out, new_state, new_hist = store(*layer(
        ep,
        hidden,
        head_input_projected,
        output_gate_projected,
        input_map_projected,
        output_map_projected,
        raw_step_size,
        jnp.swapaxes(convolution_history, 0, 1),
        convolution_kernel,
        recurrent_state_matrix,
        head_decay_rate,
        extra_log_decay,
        head_skip_weight,
        output_matrix,
        expert_norm_scale,
        token_expert_index,
        token_expert_weight,
        jnp.swapaxes(expert_gate_weight, 1, 2),
        jnp.swapaxes(expert_up_weight, 1, 2),
        expert_down_weight,
    ))
    return (layer_out, new_state, jnp.swapaxes(new_hist, 0, 1))


def solution(mesh):
    in_specs = (
        P(("grp", "ep"), "tp"),
        P(("grp", "ep"), "tp"),
        P(("grp", "ep"), "tp"),
        P(("grp", "ep"), "tp"),
        P(("grp", "ep"), "tp"),
        P(("grp", "ep"), "tp"),
        P(("grp", "ep"), None, "tp"),
        P(None, "tp"),
        P(("grp", "ep"), "tp", None, None),
        P("tp"),
        P(("grp", "ep"), "tp"),
        P("tp"),
        P("tp", None),
        P(),
        P(("grp", "ep"), None),
        P(("grp", "ep"), None),
        P("ep", None, "tp"),
        P("ep", None, "tp"),
        P("ep", "tp", None),
    )
    out_specs = (
        P(("grp", "ep"), "tp"),
        P(("grp", "ep"), "tp", None, None),
        P(("grp", "ep"), None, "tp"),
    )
    return jax.shard_map(
        functools.partial(on_device, mesh.shape["ep"]),
        mesh=mesh,
        in_specs=in_specs,
        out_specs=out_specs,
        check_vma=False,
    )
```

```python
import functools

import jax
import jax.numpy as jnp
from jax import lax
from jax.experimental import pallas as pl
from jax.experimental.pallas import tpu as pltpu
from jax.sharding import PartitionSpec as P

MESH = pl.DeviceIdType.MESH
F32 = jnp.float32
BF16 = jnp.bfloat16

STATE_DIM = 64
TOPK = 6
CAP = 2
EPSILON = 1e-06
X_SIDE = 4
FIRST = [(0, (4, -4, 3, -3, 2, -2, 1, -1))]
FAN = [(4, (4, 3, 2, 1)), (12, (-3, -2, -1))]
BLOCKS = (0, 1, 15, 2, 14, 4, 12, 3, 13, 5, 6, 7, 8, 9, 10, 11)
PLACE = {block: place for place, block in enumerate(BLOCKS)}
ORDER = (2, 1, 3)
LANES = 128
HIGH = lax.Precision.HIGHEST
VMEM_BYTES = 28 * 1024 * 1024


def iota(shape, dim):
    return lax.broadcasted_iota(jnp.int32, shape, dim)


def silu(v):
    return v / (1.0 + jnp.exp(-v))


def softplus(v):
    return jnp.maximum(v, 0.0) + jnp.log1p(jnp.exp(-jnp.abs(v)))


def layer_kernel(
    hidden_h, head_in_h, gate_h, b_map_h, c_map_h, raw_step_h, hist_h, taps_h, state_h, rate_h, extra_h, skip_h, wout_h,
    norm_h, chosen_h, weights_h, wg_h, wu_h, wd_h,
    out_h, new_state_h, new_hist_h,
    out, new_state, new_hist, hidden, head_in, gate, b_map, c_map, raw_step, hist, taps, state, rate, extra_decay, skip, wout,
    norm, chosen, weights, wg, wu, wd,
    tp_tx, tp_rx, tokens, pick_tx, pick_rx, pick_other, down_tx, down_rx, back_tx, back_rx,
    sums, sums_bf, relay_rx, relay_tx, last_rx,
    in_sem, w_sem, tp_s, tp_r, z_s, z_r, x_s, x_r, o_s, o_r, d_s, d_r, b_s, b_r, h_s, h_r,
):
    seqs, half = hidden.shape
    nz = tokens.shape[0]
    some = nz // 2
    slots = some * CAP
    rows = X_SIDE * slots
    me, core = lax.axis_index("ep"), lax.axis_index("tp")
    z, x = me // X_SIDE, me % X_SIDE
    other = 1 - core
    turn = 1 - 2 * core

    def spot(block):
        here, there = PLACE[block], PLACE[(nz - block) % nz]
        return here if here == there else jnp.where(core == 0, here, there)

    def along_z(d):
        return {"ep": ((z + turn * d + nz) % nz) * X_SIDE + x}

    def along_x(d):
        return {"ep": z * X_SIDE + (x + d) % X_SIDE}

    partner = {"tp": other}
    mine_cols = pl.ds(pl.multiple_of(core * half, half), half)
    other_cols = pl.ds(pl.multiple_of(other * half, half), half)

    pairs = [(c_map_h, c_map), (head_in_h, head_in), (hist_h, hist), (taps_h, taps), (raw_step_h, raw_step), (extra_h, extra_decay),
             (rate_h, rate), (skip_h, skip), (b_map_h, b_map), (gate_h, gate), (hidden_h, hidden), (chosen_h, chosen),
             (weights_h, weights), (norm_h, norm)]
    small = [pltpu.make_async_copy(src, dst, in_sem.at[i]) for i, (src, dst) in enumerate(pairs)]
    two = seqs // 4
    fetch = [pltpu.make_async_copy(state_h.at[pl.ds(i * two, two)], state.at[pl.ds(i * two, two)], in_sem.at[len(pairs) + i]) for i in range(4)]
    get_wout = pltpu.make_async_copy(wout_h, wout, w_sem.at[0])
    loads = [pltpu.make_async_copy(src, dst, w_sem.at[1 + i])
             for i, (src, dst) in enumerate([(wg_h.at[0], wg), (wu_h.at[0], wu), (wd_h.at[0], wd)])]
    for copy in [small[0], *fetch, *small[1:], get_wout]:
        copy.start()
    barrier = pltpu.get_barrier_semaphore()
    steps = sorted({s * h for _, hops in FIRST + FAN for h in hops for s in (1, -1)})
    peers = [along_z(h) for h in steps] + [along_x(d) for d in range(1, X_SIDE)] + [partner]
    for peer in peers:
        pl.semaphore_signal(barrier, inc=1, device_id=peer, device_id_type=MESH)

    heads = raw_step.shape[1]
    width = half // heads
    groups = b_map.shape[1] // STATE_DIM
    per_group = heads // groups
    chans = per_group * width
    small[0].wait()
    c_all = c_map[...].astype(F32)
    row_c = iota((seqs, STATE_DIM), 0)
    seen = [jnp.zeros((seqs, chans), F32) for _ in range(groups)]
    for s in range(seqs):
        if s % two == 0:
            fetch[s // two].wait()
        for g in range(groups):
            c_g = jnp.where(row_c == s, c_all[:, g * STATE_DIM : (g + 1) * STATE_DIM], 0.0).astype(BF16)
            held = state[s, g * per_group : (g + 1) * per_group].reshape(chans, STATE_DIM).astype(BF16)
            seen[g] = seen[g] + lax.dot_general(c_g, held, (((1,), (1,)), ((), ())), preferred_element_type=F32)
    for copy in small[1:]:
        copy.wait()

    fresh_in = head_in[...]
    for i in range(2):
        new_hist[i] = hist[i + 1]
    new_hist[2] = fresh_in
    kern = taps[...].astype(F32)
    total = fresh_in.astype(F32) * kern[3:4]
    for i in range(3):
        total = total + hist[i].astype(F32) * kern[i : i + 1]
    conv = silu(total)
    dt = softplus(raw_step[...].astype(F32))
    col = iota((seqs, heads), 1)
    rates = jnp.zeros((seqs, heads), F32)
    for h in range(heads):
        rates = jnp.where(col == h, rate[h], rates)
    decay = jnp.exp(-rates * dt + extra_decay[...])
    lanes_of = (iota((heads, half), 1) // width == iota((heads, half), 0)).astype(F32)
    spread = jnp.dot(jnp.concatenate([dt, decay], axis=0), lanes_of, precision=HIGH, preferred_element_type=F32)
    u = conv * spread[:seqs]
    decays = spread[seqs:]
    col = iota((seqs, half), 1) // width
    skips = jnp.zeros((seqs, half), F32)
    for h in range(heads):
        skips = jnp.where(col == h, skip[h], skips)
    opened = silu(gate[...].astype(F32))
    b_all = b_map[...].astype(F32)
    read = []
    for g in range(groups):
        cols = slice(g * STATE_DIM, (g + 1) * STATE_DIM)
        read.append(u[:, g * chans : (g + 1) * chans] * jnp.sum(b_all[:, cols] * c_all[:, cols], axis=1, keepdims=True))
    for load in loads:
        load.start()
    readout = decays * jnp.concatenate(seen, axis=1) + jnp.concatenate(read, axis=1) + skips * conv
    gated = (readout * opened).astype(BF16)

    def remote(src, dst, send, recv, peer):
        return pltpu.make_async_remote_copy(
            src_ref=src, dst_ref=dst, send_sem=send, recv_sem=recv, device_id=peer, device_id_type=MESH
        )

    idx = chosen[...]
    wts = weights[...]
    lane = iota((seqs, LANES), 1)
    named = jnp.zeros((seqs, LANES), F32)
    for i in range(TOPK):
        named = named + (lane == idx[:, i : i + 1]).astype(F32)
    before = (iota((seqs, seqs), 1) < iota((seqs, seqs), 0)).astype(BF16)
    rank = jnp.dot(before, named.astype(BF16), preferred_element_type=F32)
    extra = jnp.zeros((seqs, LANES), F32)
    for i in range(TOPK):
        expert = idx[:, i : i + 1]
        place = jnp.sum(jnp.where(lane == expert, rank, 0.0), axis=1, keepdims=True)
        slot = expert.astype(F32) * CAP + place
        w = wts[:, i : i + 1]
        w_hi = w.astype(BF16).astype(F32)
        extra = jnp.where(lane == i, slot, extra)
        extra = jnp.where(lane == TOPK + i, w_hi, extra)
        extra = jnp.where(lane == 2 * TOPK + i, w - w_hi, extra)
    tokens[0, :, half:] = extra.astype(BF16)

    get_wout.wait()
    tp_tx[...] = jnp.dot(gated, wout[:, other_cols], preferred_element_type=F32).astype(BF16)
    pl.semaphore_wait(barrier, len(peers))
    swap = remote(tp_tx, tp_rx, tp_s, tp_r, partner)
    swap.start()
    own_mix = jnp.dot(gated, wout[:, mine_cols], preferred_element_type=F32).astype(BF16)

    base = hidden[...].astype(F32)
    swap.wait()
    mixed = own_mix.astype(F32) + tp_rx[...].astype(F32)
    resid = (base + mixed).astype(BF16)
    tokens[0, :, :half] = resid

    def update_states():
        u_hi = u.astype(BF16).astype(F32)
        u_t = jnp.concatenate([u_hi, u - u_hi], axis=0).T.astype(BF16)
        row = iota((2 * seqs, STATE_DIM), 0)
        for s in range(seqs):
            for g in range(groups):
                b_g = b_all[:, g * STATE_DIM : (g + 1) * STATE_DIM]
                b_g = jnp.where(row % seqs == s, jnp.concatenate([b_g, b_g], axis=0), 0.0).astype(BF16)
                outer = jnp.dot(u_t[g * chans : (g + 1) * chans], b_g, preferred_element_type=F32)
                for j in range(per_group):
                    h = g * per_group + j
                    new_state[s, h] = decay[s : s + 1, h : h + 1] * state[s, h] + outer[j * width : (j + 1) * width]

    direct = [hop % nz for hop in FIRST[0][1] if hop % nz not in [origin for origin, _ in FAN]]

    def first_for(block):
        for i, (origin, _) in enumerate(FAN):
            if block == origin:
                return i
        return 2 if block in direct else 3

    def token_wait(count, at):
        some_blocks = tokens.at[pl.ds(0, count)]
        return remote(some_blocks, some_blocks, z_s, z_r.at[at], partner)

    def spread_from(origin, hops):
        for hop in hops:
            lands = (origin + hop) % nz
            remote(tokens.at[spot(origin)], tokens.at[spot(lands)], z_s, z_r.at[first_for(lands)], along_z(hop)).start()

    for origin, hops in FIRST:
        spread_from(origin, hops)
    update_states()
    keep = [pltpu.make_async_copy(new_state, new_state_h, w_sem.at[4]), pltpu.make_async_copy(new_hist, new_hist_h, w_sem.at[5]),
            pltpu.make_async_copy(out, out_h, w_sem.at[6])]
    for copy in keep[:2]:
        copy.start()
    for origin, hops in FAN:
        token_wait(1, first_for(origin)).wait_recv()
        spread_from(origin, hops)

    def at_x(ref, part, d):
        return ref.at[part, (x + d + X_SIDE) % X_SIDE]

    def across(part):
        if part:
            token_wait(nz - 1 - len(FAN) - len(direct), 3).wait_recv()
        else:
            token_wait(len(direct), 2).wait_recv()
        held = tokens[part * some : (part + 1) * some].astype(F32).reshape(some * seqs, half + LANES)
        info = held[:, half:]
        info = info + jnp.where(iota(info.shape, 1) < TOPK, 0.0, pltpu.roll(info, LANES - TOPK, 1))
        shape = (some * seqs, X_SIDE * slots)
        col = iota(shape, 1)
        slot_of = ((z * X_SIDE + col // slots) * CAP + col % CAP).astype(F32)
        same_z = (col % slots) // CAP == iota(shape, 0) // seqs
        takes = jnp.zeros(shape, F32)
        mixing = jnp.zeros(shape, F32)
        for i in range(TOPK):
            hit = same_z & (info[:, i : i + 1] == slot_of)
            takes = jnp.where(hit, 1.0, takes)
            mixing = jnp.where(hit, info[:, TOPK + i : TOPK + i + 1], mixing)
        mix_hi = mixing.astype(BF16)
        mix_lo = (mixing - mix_hi.astype(F32)).astype(BF16)
        picked = jnp.dot(takes.T.astype(BF16), held[:, :half].astype(BF16), preferred_element_type=F32).astype(BF16)
        pick_tx[part] = picked.reshape(X_SIDE, slots, half)
        sent = []
        for i, d in enumerate(ORDER):
            sent.append(remote(at_x(pick_tx, part, d), pick_rx.at[part, x], x_s.at[part], x_r.at[part, i], along_x(d)))
            sent[i].start()
        pick_rx[part, x] = pick_tx[part, x]
        shared = [remote(pick_tx.at[part, x], pick_other.at[part, x], o_s.at[part], o_r.at[part], partner)]
        shared[0].start()
        return sent, shared, (mix_hi, mix_lo)

    def share(part, shared):
        for i in (1, 2, 0):
            d = ORDER[i]
            got = at_x(pick_rx, part, -d)
            remote(got, got, x_s.at[part], x_r.at[part, i], along_x(d)).wait_recv()
            shared.append(remote(got, at_x(pick_other, part, -d), o_s.at[part], o_r.at[part], partner))
            shared[-1].start()

    def project(values, cols):
        f = values.reshape(rows, half).astype(F32)
        scaled = (f * norm[cols].astype(F32)[None, :]).astype(BF16)
        dims = (((1,), (1,)), ((), ()))
        g = lax.dot_general(scaled, wg[:, cols], dims, preferred_element_type=F32)
        u = lax.dot_general(scaled, wu[:, cols], dims, preferred_element_type=F32)
        return g, u, jnp.sum(f * f, axis=1, keepdims=True)

    def activate(part, shared):
        g0, u0, s0 = project(pick_rx[part], mine_cols)
        remote(pick_rx.at[part], pick_other.at[part], o_s.at[part], o_r.at[part], partner).wait_recv()
        g1, u1, s1 = project(pick_other[part], other_cols)
        inv = lax.rsqrt((s0 + s1) / (2 * half) + EPSILON)
        return (silu(inv * (g0 + g1)) * (inv * (u0 + u1))).astype(BF16)

    def down(part, act):
        down_tx[part] = jnp.dot(act, wd[:, other_cols], preferred_element_type=F32).astype(BF16)
        trade = remote(down_tx.at[part], down_rx.at[part], d_s.at[part], d_r.at[part], partner)
        trade.start()
        return trade, jnp.dot(act, wd[:, mine_cols], preferred_element_type=F32).astype(BF16)

    def back(part, trade, own_down):
        trade.wait_recv()
        result = (own_down.astype(F32) + down_rx[part].astype(F32)).astype(BF16)
        back_tx[part] = result.reshape(X_SIDE, slots, half)
        returned = []
        for i, d in enumerate(ORDER):
            returned.append(remote(at_x(back_tx, part, d), back_rx.at[part, x], b_s.at[part], b_r.at[part], along_x(d)))
            returned[i].start()
        back_rx[part, x] = back_tx[part, x]
        return returned

    def three_backs(part):
        blocks = pl.ds(0, X_SIDE - 1)
        return remote(back_tx.at[part, blocks], back_rx.at[part, blocks], b_s.at[part], b_r.at[part], partner)

    def collect(part, mix):
        three_backs(part).wait_recv()
        rows_back = back_rx[part].reshape(rows, half)
        total = jnp.dot(mix[0], rows_back, preferred_element_type=F32) + jnp.dot(mix[1], rows_back, preferred_element_type=F32)
        total = total.reshape(some, seqs, half)
        sums[part * some : (part + 1) * some] = total
        sums_bf[part * some : (part + 1) * some] = total.astype(BF16)

    sent_n, shared_n, mix_n = across(0)
    sent_f, shared_f, mix_f = across(1)
    share(0, shared_n)
    for load in loads:
        load.wait()
    act_n = activate(0, shared_n)
    share(1, shared_f)
    act_f = activate(1, shared_f)
    trade_f, own_f = down(1, act_f)
    trade_n, own_n = down(0, act_n)
    returned_f = back(1, trade_f, own_f)
    returned_n = back(0, trade_n, own_n)

    def send(src, dst, hop, at):
        remote(src, dst, h_s, h_r.at[at], along_z(hop)).start()

    def sum_wait(count, at):
        some_blocks = sums_bf.at[pl.ds(0, count)]
        return remote(some_blocks, some_blocks, h_s, h_r.at[at], partner)

    (_, first_hops), = FIRST
    counts = [len(hops) for _, hops in FAN]

    collect(1, mix_f)
    for i, (origin, hops) in enumerate(FAN):
        for n, hop in enumerate(hops):
            send(sums_bf.at[spot((origin + hop) % nz)], relay_rx.at[sum(counts[:i]) + n], -hop, i)
    collect(0, mix_n)
    for i, (origin, hops) in enumerate(FAN):
        sum_wait(counts[i], i).wait_recv()
        total = sums[spot(origin)]
        for n in range(counts[i]):
            total = total + relay_rx[sum(counts[:i]) + n].astype(F32)
        relay_tx[i] = total.astype(BF16)
        send(relay_tx.at[i], last_rx.at[i], -first_hops[i], 2)
    for i, hop in enumerate(first_hops[len(FAN) :]):
        send(sums_bf.at[spot(hop % nz)], last_rx.at[len(FAN) + i], -hop, 2)
    total = resid.astype(F32) + sums[0]
    sum_wait(len(first_hops), 2).wait_recv()
    for i in range(len(first_hops)):
        total = total + last_rx[i].astype(F32)
    out[...] = total.astype(BF16)
    keep[2].start()
    token_wait(nz - 1, 0).wait_send()
    sum_wait(nz - 1, 0).wait_send()
    for part in range(2):
        three = pick_tx.at[part, pl.ds(0, X_SIDE - 1)]
        remote(three, three, x_s.at[part], x_r.at[part, 0], partner).wait_send()
        remote(pick_rx.at[part], pick_other.at[part], o_s.at[part], o_r.at[part], partner).wait_send()
        three_backs(part).wait_send()
    trade_n.wait_send()
    trade_f.wait_send()
    for copy in keep:
        copy.wait()


def layer(ep, *args):
    hidden, head_in, gate, b_map, c_map, raw_step, hist, taps, state, rate, extra, skip, wout, norm, chosen, weights, wg, wu, wd = args
    seqs, half = hidden.shape
    nz = ep // X_SIDE
    slots = nz // 2 * CAP
    rows = X_SIDE * slots
    far = sum(len(hops) for _, hops in FAN)
    near = len(FIRST[0][1])
    vmem = pl.BlockSpec(memory_space=pltpu.VMEM)
    hbm = pl.BlockSpec(memory_space=pltpu.HBM)
    dma = pltpu.SemaphoreType.DMA
    one = dma(())

    def room(a):
        return pltpu.VMEM(a.shape, a.dtype)

    return pl.pallas_call(
        layer_kernel,
        name="layer",
        in_specs=[hbm] * len(args),
        out_specs=[pl.BlockSpec(memory_space=pl.ANY)] * 3,
        out_shape=[
            pltpu.VMEM(hidden.shape, BF16),
            pltpu.VMEM(state.shape, F32),
            pltpu.VMEM(hist.shape, BF16),
        ],
        scratch_shapes=[
            room(hidden),
            room(state),
            room(hist),
            *(pltpu.SMEM(a.shape, F32) if a is rate or a is skip else room(a) for a in args[:16]),
            *(pltpu.VMEM(a.shape[1:], BF16) for a in (wg, wu, wd)),
            room(hidden),
            room(hidden),
            pltpu.VMEM((nz, seqs, half + LANES), BF16),
            *(pltpu.VMEM((2, X_SIDE, slots, half), BF16) for _ in range(3)),
            *(pltpu.VMEM((2, rows, half), BF16) for _ in range(2)),
            *(pltpu.VMEM((2, X_SIDE, slots, half), BF16) for _ in range(2)),
            pltpu.VMEM((nz, seqs, half), F32),
            pltpu.VMEM((nz, seqs, half), BF16),
            pltpu.VMEM((far, seqs, half), BF16),
            pltpu.VMEM((2, seqs, half), BF16),
            pltpu.VMEM((near, seqs, half), BF16),
            dma((14 + 4,)), dma((7,)), one, one, one, dma((4,)), dma((2,)), dma((2, 3)), dma((2,)), dma((2,)),
            dma((2,)), dma((2,)), dma((2,)), dma((2,)), one, dma((3,)),
        ],
        compiler_params=pltpu.CompilerParams(collective_id=0, has_side_effects=True, vmem_limit_bytes=VMEM_BYTES),
    )(*(pltpu.with_memory_space_constraint(a, pltpu.HBM) for a in args))


def store_kernel(*refs):
    count = (len(refs) - 1) // 2
    pairs = list(zip(refs[:count], refs[count:-1]))
    for at, (src, dst) in enumerate(pairs):
        pieces = src.shape[0] if src.ndim == 4 else 1
        for i in range(pieces):
            piece = pl.ds(i * (src.shape[0] // pieces), src.shape[0] // pieces)
            pltpu.make_async_copy(src.at[piece], dst.at[piece], refs[-1].at[at]).start()
    for at, (src, dst) in enumerate(pairs):
        pltpu.make_async_copy(src, dst, refs[-1].at[at]).wait()


def store(*values):
    return pl.pallas_call(
        store_kernel,
        name="store",
        in_specs=[pl.BlockSpec(memory_space=pl.ANY)] * len(values),
        out_specs=[pl.BlockSpec(memory_space=pltpu.HBM)] * len(values),
        out_shape=[pltpu.HBM(v.shape, v.dtype) for v in values],
        scratch_shapes=[pltpu.SemaphoreType.DMA((len(values),))],
        compiler_params=pltpu.CompilerParams(vmem_limit_bytes=VMEM_BYTES),
    )(*(pltpu.with_memory_space_constraint(v, pltpu.VMEM) for v in values))


def on_device(
    ep,
    hidden,
    head_input_projected,
    output_gate_projected,
    input_map_projected,
    output_map_projected,
    raw_step_size,
    convolution_history,
    convolution_kernel,
    recurrent_state_matrix,
    head_decay_rate,
    extra_log_decay,
    head_skip_weight,
    output_matrix,
    expert_norm_scale,
    token_expert_index,
    token_expert_weight,
    expert_gate_weight,
    expert_up_weight,
    expert_down_weight,
):
    layer_out, new_state, new_hist = store(*layer(
        ep,
        hidden,
        head_input_projected,
        output_gate_projected,
        input_map_projected,
        output_map_projected,
        raw_step_size,
        jnp.swapaxes(convolution_history, 0, 1),
        convolution_kernel,
        recurrent_state_matrix,
        head_decay_rate,
        extra_log_decay,
        head_skip_weight,
        output_matrix,
        expert_norm_scale,
        token_expert_index,
        token_expert_weight,
        jnp.swapaxes(expert_gate_weight, 1, 2),
        jnp.swapaxes(expert_up_weight, 1, 2),
        expert_down_weight,
    ))
    return (layer_out, new_state, jnp.swapaxes(new_hist, 0, 1))


def solution(mesh):
    in_specs = (
        P(("grp", "ep"), "tp"),
        P(("grp", "ep"), "tp"),
        P(("grp", "ep"), "tp"),
        P(("grp", "ep"), "tp"),
        P(("grp", "ep"), "tp"),
        P(("grp", "ep"), "tp"),
        P(("grp", "ep"), None, "tp"),
        P(None, "tp"),
        P(("grp", "ep"), "tp", None, None),
        P("tp"),
        P(("grp", "ep"), "tp"),
        P("tp"),
        P("tp", None),
        P(),
        P(("grp", "ep"), None),
        P(("grp", "ep"), None),
        P("ep", None, "tp"),
        P("ep", None, "tp"),
        P("ep", "tp", None),
    )
    out_specs = (
        P(("grp", "ep"), "tp"),
        P(("grp", "ep"), "tp", None, None),
        P(("grp", "ep"), None, "tp"),
    )
    return jax.shard_map(
        functools.partial(on_device, mesh.shape["ep"]),
        mesh=mesh,
        in_specs=in_specs,
        out_specs=out_specs,
        check_vma=False,
    )
```
